512 devices in a mesh: sp: 32 (over z, x), dp: 16 (over y, core).
Axes of the slice: x: 4, y: 8, z: 8, core: 2. Of those that a mesh axis runs over, the one named last changes fastest.
Arguments:
- query_rows: bfloat16 [16, 4096, 2048], P('dp', 'sp'), may hold values from -6 to 6
- key_rows: bfloat16 [16, 4096, 2048], P('dp', 'sp'), may hold values from -6 to 6
- value_rows: bfloat16 [16, 4096, 2048], P('dp', 'sp'), may hold values from -6 to 6
- decay_low: bfloat16 [16, 4096, 128], P('dp', 'sp'), may hold values from -5 to 5
- rate_low: bfloat16 [16, 4096, 128], P('dp', 'sp'), may hold values from -4 to 4
- decay_up: bfloat16 [128, 2048], replicated, may hold values from -0.5 to 0.5
- rate_up: bfloat16 [128, 2048], replicated, may hold values from -0.5 to 0.5
- decay_base: float32 [2048], replicated, may hold values from -12 to -2
- norm_gain: float32 [2048], replicated, may hold values from 0.1 to 1.9
- out_weight: bfloat16 [2048, 2048], P(None, 'dp'), may hold values from -0.125 to 0.125
Outputs:
- layer_out: bfloat16 [16, 4096, 2048], P('dp', 'sp')
The draws below stay inside these ranges and needn't reach their ends.
All inputs are finite; a program needn't handle non-finite values.
Results may differ from the reference program's by a relative error of at most 0.005.
Values may be sent and summed in bfloat16 or wider, within the bound.
A program may use at most 128 MiB of HBM per device.

```python
import jax
import jax.numpy as jnp
from jax import lax

D = 2048
HEADS = 32
HEAD = 64
LOW = 128
TOK_DEV = 128
WIDTH = 2048
LENGTH = 4096
BATCH = 16


def draw_decay_low(key, part):
    noise = jnp.clip(jax.random.normal(jax.random.fold_in(key, 11), (BATCH, LENGTH, LOW), jnp.float32), -4.0, 4.0)
    offsets = jax.random.uniform(jax.random.fold_in(key, 12), (BATCH, LENGTH // TOK_DEV, 1), jnp.float32, minval=-1.0, maxval=1.0)
    total = noise + jnp.repeat(offsets, TOK_DEV, axis=1)
    return jnp.clip(total, -5.0, 5.0).astype(jnp.bfloat16)


def draw_decay_base(key, part):
    picks = jax.random.randint(jax.random.fold_in(key, 21), (HEADS, 1), 0, 16)
    quick = picks < 8
    slow_rate = jax.random.uniform(jax.random.fold_in(key, 22), (HEADS, HEAD), jnp.float32, minval=0.2, maxval=1.0) / LENGTH
    quick_rate = jax.random.uniform(jax.random.fold_in(key, 23), (HEADS, HEAD), jnp.float32, minval=0.01, maxval=0.033)
    chosen = jnp.where(quick, quick_rate, slow_rate)
    return jnp.clip(jnp.log(chosen) + 0.5, -12.0, -2.0).reshape(WIDTH).astype(jnp.float32)


def block_levels(key, extent, pieces, least, top_value):
    level = 1.0
    for dim, parts in pieces:
        heights = jax.random.uniform(jax.random.fold_in(jax.random.fold_in(key, 6), dim), (parts,), jnp.float32, least / len(pieces), top_value / len(pieces))
        level = level * jnp.repeat(jnp.exp(heights), extent[dim] // parts).reshape((-1,) + (1,) * (len(extent) - 1 - dim))
    return level


def gaussian(stream_key, dims, deviation, reach, cuts=(), held_as=jnp.bfloat16):
    values = deviation * jax.random.normal(stream_key, dims, jnp.float32)
    if cuts:
        values = values * block_levels(stream_key, dims, cuts, -0.22, 0.18)
    return jnp.clip(values, -reach, reach).astype(held_as)


def setup_inputs(seed: int = 0) -> dict:
    splits = jax.random.split(jax.random.key(seed), 11)
    query_rows = gaussian(splits[0], (BATCH, LENGTH, WIDTH), 1.0, 6.0, ((0, 16), (1, 32)))
    key_rows = gaussian(splits[1], (BATCH, LENGTH, WIDTH), 1.0, 6.0, ((0, 16), (1, 32)))
    value_rows = gaussian(splits[2], (BATCH, LENGTH, WIDTH), 1.0, 6.0, ((0, 16), (1, 32)))
    decay_low = draw_decay_low(jax.random.fold_in(splits[10], 71), 0)
    rate_low = gaussian(splits[4], (BATCH, LENGTH, LOW), 1.0, 4.0, ((0, 16), (1, 32)))
    decay_up = gaussian(splits[5], (LOW, WIDTH), LOW ** -0.5, 0.5)
    rate_up = gaussian(splits[6], (LOW, WIDTH), LOW ** -0.5, 0.5)
    decay_base = draw_decay_base(jax.random.fold_in(splits[10], 71), 0)
    norm_gain = jnp.clip(1.0 + 0.18 * jax.random.normal(splits[8], (WIDTH,), jnp.float32), 0.1, 1.9)
    out_weight = gaussian(splits[9], (WIDTH, D), WIDTH ** -0.5, 0.125, ((1, 16),))
    return {"query_rows": query_rows, "key_rows": key_rows, "value_rows": value_rows, "decay_low": decay_low, "rate_low": rate_low, "decay_up": decay_up, "rate_up": rate_up, "decay_base": decay_base, "norm_gain": norm_gain, "out_weight": out_weight}


HIGHEST = lax.Precision.HIGHEST

def reference(query_rows, key_rows, value_rows, decay_low, rate_low, decay_up, rate_up, decay_base, norm_gain, out_weight):
    heads = query_rows.shape[2] // HEAD

    def one_sequence(inputs):
        reads, keyed, valued, low_decay, low_rate = inputs
        positions = reads.shape[0]
        squashed = jnp.tanh(low_decay.astype(jnp.float32)).astype(jnp.bfloat16)
        decay_pre = (decay_base + jnp.dot(squashed, decay_up, preferred_element_type=jnp.float32)).astype(jnp.bfloat16)
        rate_pre = jnp.dot(low_rate, rate_up, preferred_element_type=jnp.float32).astype(jnp.bfloat16)
        log_decay = -jnp.exp(-jax.nn.softplus(-decay_pre.astype(jnp.float32)) - 0.5)
        rate = jax.nn.sigmoid(rate_pre.astype(jnp.float32))
        head_shape = (positions, heads, HEAD)
        query_heads = reads.astype(jnp.float32).reshape(head_shape)
        key_heads = keyed.astype(jnp.float32).reshape(head_shape)
        value_heads = valued.astype(jnp.float32).reshape(head_shape)
        decay_heads = jnp.exp(log_decay).reshape(head_shape)
        unit_keys = key_heads * lax.rsqrt(1.0 + lax.optimization_barrier(jnp.sum(key_heads * key_heads, axis=-1, keepdims=True)))
        erase = unit_keys * rate.reshape(head_shape)

        def advance(state, inputs_now):
            query_now, decay_now, key_now, value_now, unit_now, erase_now = inputs_now
            removed = jnp.einsum('hvk,hk->hv', state, unit_now, precision=HIGHEST)
            state = state * decay_now[:, None, :] - removed[:, :, None] * erase_now[:, None, :] + value_now[:, :, None] * key_now[:, None, :]
            return (state, jnp.einsum('hvk,hk->hv', state, query_now, precision=HIGHEST))
        initial = jnp.zeros((heads, HEAD, HEAD), jnp.float32)
        _, readout = lax.scan(advance, initial, (query_heads, decay_heads, key_heads, value_heads, unit_keys, erase))
        average = lax.optimization_barrier(jnp.mean(readout, axis=-1, keepdims=True))
        centred = readout - average
        variance = lax.optimization_barrier(jnp.mean(centred * centred, axis=-1, keepdims=True))
        normed = (centred * lax.rsqrt(variance + 1.0)).reshape(positions, heads * HEAD)
        mix = (normed * norm_gain).astype(jnp.bfloat16)
        return jnp.dot(mix, out_weight, preferred_element_type=jnp.float32).astype(jnp.bfloat16)
    return lax.map(one_sequence, (query_rows, key_rows, value_rows, decay_low, rate_low))
```

```python
import jax
import jax.numpy as jnp
from jax import lax
from jax.experimental import pallas as pl
from jax.experimental.pallas import tpu as pltpu
from jax.sharding import PartitionSpec as P

F32 = jnp.float32
BF16 = jnp.bfloat16
C = 128
PAIRS = 16
SP = 32
DPN = 16
YN = 8
MSG = 80
DECAY_SCALE = 0.6065306597126334
MESH = pl.DeviceIdType.MESH


def split(x):
    high = x.astype(BF16)
    return high, (x - high.astype(F32)).astype(BF16)


def nn(a, b):
    return jnp.dot(a, b, preferred_element_type=F32)


def nt(a, b):
    return lax.dot_general(a, b, (((1,), (1,)), ((), ())), preferred_element_type=F32)


def rows_of(*parts):
    return jnp.concatenate(parts, axis=0)


def lanes_of(*parts):
    return jnp.concatenate(parts, axis=1)


def sigmoid(x):
    return 1.0 / (1.0 + jnp.exp(-x))


def iotas():
    return (
        lax.broadcasted_iota(jnp.int32, (C, C), 0),
        lax.broadcasted_iota(jnp.int32, (C, C), 1),
    )


def roll_half(x):
    return pltpu.roll(x, 64, 1)


def pair_front(pair, q_ref, k_ref, v_ref, sq_ref, rl_ref, du_ref, ru_ref, base_ref):
    row, col = iotas()
    first = col < 64
    at = pl.ds(pl.multiple_of(pair * C, C), C)
    decay_pre = (base_ref[pl.ds(pair, 1), :] + nn(sq_ref[...], du_ref[:, at])).astype(BF16).astype(F32)
    rate_pre = nn(rl_ref[...], ru_ref[:, at]).astype(BF16).astype(F32)
    log_decay = -DECAY_SCALE * sigmoid(decay_pre)
    rate = sigmoid(rate_pre)
    tri = jnp.where(row >= col, 1.0, 0.0).astype(BF16)
    ld_h, ld_l = split(log_decay)
    running = nn(lanes_of(tri, tri), rows_of(ld_h, ld_l))
    key = k_ref[:, at].astype(F32)
    query = q_ref[:, at].astype(F32)
    same = jnp.where((row < 64) == first, 1.0, 0.0).astype(BF16)
    sq_h, sq_l = split(key * key)
    unit = key * lax.rsqrt(1.0 + nn(lanes_of(sq_h, sq_l), rows_of(same, same)))
    erase = unit * rate
    centre = running[63:64, :]
    final = running[C - 1 : C, :]
    up = jnp.exp(running - centre)
    down = jnp.exp(centre - running)
    before = jnp.exp(running - log_decay - centre)
    from_start = jnp.exp(centre)
    to_end = jnp.exp(final - centre)
    f1 = unit * before
    f2 = query * up
    g1 = key * down
    g2 = erase * down
    return f1, f2, g1, g2, f1 * from_start, f2 * from_start, g1 * to_end, g2 * to_end, jnp.exp(final)


def pair_body(pair, refs, msg_ref, p_ref, o_ref):
    q_ref, k_ref, v_ref, sq_ref, rl_ref, du_ref, ru_ref, base_ref = refs
    row, col = iotas()
    first = col < 64
    first_b = lax.broadcasted_iota(jnp.int32, (2 * C, C), 1) < 64
    strict = row > col
    within = row >= col
    at = pl.ds(pl.multiple_of(pair * C, C), C)
    f1, f2, g1, g2, es, qs, ke, ee, efin = pair_front(pair, *refs)
    f_h, f_l = split(rows_of(f1, f2))
    zero2 = jnp.zeros((2 * C, C), BF16)
    fa_h, fa_l = jnp.where(first_b, f_h, zero2), jnp.where(first_b, f_l, zero2)
    fb_h, fb_l = jnp.where(first_b, zero2, f_h), jnp.where(first_b, zero2, f_l)
    g_h, g_l = split(rows_of(g1, g2))
    gg = lanes_of(g_h, g_h)
    grams = [
        nt(lanes_of(fa_h, fa_l), gg) + nt(fa_h, g_l),
        nt(lanes_of(fb_h, fb_l), gg) + nt(fb_h, g_l),
    ]
    v_roll = roll_half(v_ref[:, at].astype(F32)).astype(BF16)
    zero1 = jnp.zeros((C, C), BF16)
    eye = jnp.where(row == col, 1.0, 0.0)
    ep, kp, rk, re, x = [], [], [], [], []
    differ = row ^ col
    for g in grams:
        kp.append(split(jnp.where(strict, g[:C, :C], 0.0)))
        ep.append(split(jnp.where(strict, g[:C, C:], 0.0)))
        rk.append(split(jnp.where(within, g[C:, :C], 0.0)))
        re.append(split(jnp.where(within, g[C:, C:], 0.0)))
        x.append(eye - jnp.where(differ == 1, ep[-1][0].astype(F32), 0.0))
    size = 2
    while size < C:
        level = (differ >= size) & (differ < 2 * size)
        xb = [a.astype(BF16) for a in x]
        mid = [nn(xb[i], jnp.where(level, ep[i][0], zero1)).astype(BF16) for i in range(2)]
        x = [x[i] - nn(mid[i], xb[i]) for i in range(2)]
        size *= 2
    ee_t = split(ee.T)
    ke_t = split(ke.T)
    outs = []
    for i in range(2):
        mine = first if i == 0 else ~first
        xb = x[i].astype(BF16)
        carried = nn(lanes_of(*kp[i]), rows_of(v_roll, v_roll))
        rhs = jnp.where(mine, es, carried)
        s0 = nn(xb, rhs.astype(BF16)).astype(BF16)
        resid = rhs - s0.astype(F32) - nn(lanes_of(*ep[i]), rows_of(s0, s0))
        sol = s0.astype(F32) + nn(xb, resid.astype(BF16))
        n_h, n_l = split(-sol)
        v_mine = jnp.where(mine, zero1, v_roll)
        w_h = rows_of(n_h, v_mine)
        half = slice(64 * i, 64 * i + 64)
        l_h = rows_of(lanes_of(ee_t[0][half], ke_t[0][half]), lanes_of(re[i][0], rk[i][0]))
        l_l = rows_of(lanes_of(ee_t[1][half], ke_t[1][half]), lanes_of(re[i][1], rk[i][1]))
        outs.append(nn(l_h, w_h) + nn(l_l, w_h) + nn(rows_of(ee_t[0][half], re[i][0]), n_l))
    d_h, d_l = split(jnp.broadcast_to(efin, (16, C)))
    low_rows = lax.broadcasted_iota(jnp.int32, (16, C), 0) < 8
    d_tile = jnp.where(low_rows, d_h, d_l)
    for i in range(2):
        msg_ref[2 * pair + i, pl.ds(0, 64), :] = outs[i][:64].astype(BF16)
        msg_ref[2 * pair + i, pl.ds(64, 16), :] = d_tile
    p_all = qs + jnp.where(first, outs[0][64:], outs[1][64:])
    o_all = roll_half(jnp.where(first, outs[1][64:], outs[0][64:]))
    p_h, p_l = split(p_all)
    p_ref[pair] = lanes_of(p_h, p_l)
    o_ref[pair] = o_all


def compose_chunks(odd, msg_ref, zs_ref, g_ref):
    row = lax.broadcasted_iota(jnp.int32, (64, C), 0)
    col = lax.broadcasted_iota(jnp.int32, (64, C), 1)
    left = col < 64
    groups, per = 4, 8
    state = [jnp.where(row == col, 1.0, 0.0) for _ in range(groups)]
    zero = jnp.zeros((64, C), BF16)
    for step in range(per):
        for g in range(groups):
            c = g * per + step
            g_ref[g, pl.ds(64 * step, 64), :] = state[g]
            m = msg_ref[c, pl.ds(0, 64), :].astype(F32)
            tile = msg_ref[c, pl.ds(64, 16), :].astype(F32)
            d = tile[0:1, :] + tile[8:9, :]
            m = jnp.where(odd, roll_half(m), m)
            d = jnp.where(odd, roll_half(jnp.broadcast_to(d, (8, C)))[0:1, :], d)
            trans = jnp.where(left, m + jnp.where(row == col, d, 0.0), 0.0)
            add = jnp.where(left, 0.0, m)
            t_h, t_l = split(trans)
            lhs = lanes_of(jnp.where(left, t_h.astype(F32), roll_half(t_l.astype(F32))).astype(BF16), t_h)
            s_h, s_l = split(state[g])
            state[g] = nn(lhs, rows_of(s_h, s_h, s_l, zero)) + add
    starts = [None]
    z = jnp.where(left, roll_half(state[0]), 0.0)
    for g in range(1, groups):
        starts.append(z)
        if g < groups - 1:
            z = jnp.where(left, apply_state(state[g], z, left) + roll_half(state[g]), 0.0)
    for g in range(groups):
        stack = g_ref[g]
        wide = lax.broadcasted_iota(jnp.int32, (64 * per, C), 1) < 64
        total = roll_half(stack)
        if g > 0:
            total = total + apply_state(stack, starts[g], wide)
        for step in range(per):
            zc = total[64 * step : 64 * step + 64]
            packed = jnp.where(left[:32], zc[:32], roll_half(zc[32:]))
            zs_ref[g * per + step] = packed.astype(BF16)


def apply_state(stack, z, left):
    t_h, t_l = split(jnp.where(left, stack, 0.0))
    z_h, z_l = split(z)
    zero = jnp.zeros((64, C), BF16)
    lhs = lanes_of(jnp.where(left, t_h.astype(F32), roll_half(t_l.astype(F32))).astype(BF16), t_h)
    return nn(lhs, rows_of(z_h, z_h, z_l, zero))


def pair_finish(pair, z_ref, p_ref, o_ref, gain_ref, mix_ref):
    row, col = iotas()
    left = lax.broadcasted_iota(jnp.int32, (32, C), 1) < 64
    za = z_ref[2 * pair].astype(F32)
    zb = z_ref[2 * pair + 1].astype(F32)
    zw = rows_of(
        jnp.where(left, za, 0.0),
        jnp.where(left, roll_half(za), 0.0),
        jnp.where(left, 0.0, roll_half(zb)),
        jnp.where(left, 0.0, zb),
    ).astype(BF16)
    read = o_ref[pair] + nn(p_ref[pair], rows_of(zw, zw))
    mean_w = jnp.where((row < 64) == (col < 64), 1.0 / 64, 0.0).astype(BF16)
    mean_w = rows_of(mean_w, mean_w)
    centred = read - nn(lanes_of(*split(read)), mean_w)
    var = nn(lanes_of(*split(centred * centred)), mean_w)
    at = pl.ds(pl.multiple_of(pair * C, C), C)
    mix_ref[:, at] = (centred * lax.rsqrt(var + 1.0) * gain_ref[pl.ds(pair, 1), :]).astype(BF16)


def project(mix_ref, w_ref, out_ref):
    @pl.loop(0, YN)
    def _(y):
        acc = jnp.zeros((C, 2 * C), F32)
        for k in range(8):
            w = lanes_of(w_ref[2 * y, pl.ds(256 * k, 256), :], w_ref[2 * y + 1, pl.ds(256 * k, 256), :])
            acc = acc + nn(mix_ref[:, pl.ds(256 * k, 256)], w)
        out_ref[:, pl.ds(pl.multiple_of(y * 256, 256), 256)] = acc.astype(BF16)


def remote(src, dst, send, recv, **where):
    return pltpu.make_async_remote_copy(
        src_ref=src, dst_ref=dst, send_sem=send, recv_sem=recv, device_id=where, device_id_type=MESH
    )


def kernel(
    q_ref,
    k_ref,
    v_ref,
    dl_ref,
    rl_ref,
    du_ref,
    ru_ref,
    base_ref,
    gain_ref,
    w_ref,
    out_ref,
    sq_ref,
    msg_ref,
    got_ref,
    group_ref,
    zs_ref,
    zgot_ref,
    p_ref,
    o_ref,
    mix_ref,
    wall_ref,
    own_sem,
    msg_send,
    msg_recv,
    z_send,
    z_recv,
    ring_send,
    ring_recv,
    side_send,
    side_recv,
):
    me = lax.axis_index("sp")
    dp = lax.axis_index("dp")
    core = lax.rem(dp, 2)
    chip = lax.div(dp, 2)
    partner = dp + 1 - 2 * core
    up = lax.rem(dp + 2, DPN)
    down = lax.rem(dp + DPN - 2, DPN)

    barrier = pltpu.get_barrier_semaphore()

    @pl.loop(1, SP)
    def _(j):
        pl.semaphore_signal(
            barrier, inc=1, device_id={"sp": lax.rem(me + j, SP)}, device_id_type=MESH
        )

    for other in (partner, up, down):
        pl.semaphore_signal(barrier, inc=1, device_id={"dp": other}, device_id_type=MESH)
    own = pltpu.make_async_copy(w_ref, wall_ref.at[dp], own_sem)
    own.start()
    sq_ref[...] = jnp.tanh(dl_ref[...].astype(F32)).astype(BF16)
    own.wait()
    pl.semaphore_wait(barrier, SP + 2)

    def piece(column, half):
        return wall_ref.at[column, pl.ds(half * 1024, 1024), :]

    def ring(way, order, column, half):
        ref = piece(column, half)
        return remote(ref, ref, ring_send.at[way, order], ring_recv.at[way, order], dp=(up, down)[way])

    def side(slot, column, half):
        ref = piece(column, half)
        return remote(ref, ref, side_send.at[slot], side_recv.at[slot], dp=partner)

    for order in range(2):
        ring(0, order, dp, order).start()
        ring(1, order, dp, 1 - order).start()
        side(14 + order, dp, order).start()

    def ring_step(s):
        near = lax.div(s, 2) + 1
        half0 = lax.rem(s, 2)
        for way in range(2):
            half = half0 if way == 0 else 1 - half0
            column = lax.rem(chip + (YN - near if way == 0 else near), YN) * 2 + core
            ring(way, s, column, half).wait_recv()

            @pl.when(s < 5)
            def _():
                ring(way, s + 2, column, half).start()

            side(2 * s + way, column, half).start()

    def send_message(head):
        return remote(
            msg_ref.at[head], got_ref.at[me], msg_send.at[head], msg_recv.at[me], sp=head
        )

    def send_pair(pair):
        for i in range(2):
            head = 2 * pair + i

            @pl.when(head != me)
            def _():
                send_message(head).start()

    first_pair = lax.div(me, 2)
    refs = (q_ref, k_ref, v_ref, sq_ref, rl_ref, du_ref, ru_ref, base_ref)

    @pl.loop(0, PAIRS)
    def _(i):
        pair = lax.rem(first_pair + i, PAIRS)

        @pl.when(i > 0)
        def _():
            send_pair(lax.rem(first_pair + i + PAIRS - 1, PAIRS))

        @pl.when((i >= 2) & (lax.rem(i, 2) == 0))
        def _():
            ring_step(lax.div(i, 2) - 1)

        pair_body(pair, refs, msg_ref, p_ref, o_ref)

    got_ref[me] = msg_ref[me]
    send_pair(lax.rem(first_pair + PAIRS - 1, PAIRS))

    @pl.loop(1, SP)
    def _(j):
        other = lax.rem(me + j, SP)
        remote(
            msg_ref.at[me], got_ref.at[other], msg_send.at[other], msg_recv.at[other], sp=other
        ).wait_recv()

    compose_chunks(lax.rem(me, 2) == 1, got_ref, zs_ref, group_ref)

    def send_state(chunk):
        return remote(
            zs_ref.at[chunk], zgot_ref.at[me], z_send.at[chunk], z_recv.at[me], sp=chunk
        )

    zgot_ref[me] = zs_ref[me]

    @pl.loop(1, SP)
    def _(j):
        send_state(lax.rem(me + j, SP)).start()

    @pl.loop(1, SP)
    def _(j):
        other = lax.rem(me + SP - j, SP)
        remote(
            zs_ref.at[me], zgot_ref.at[other], z_send.at[other], z_recv.at[other], sp=other
        ).wait_recv()

    @pl.loop(0, PAIRS)
    def _(i):
        pair_finish(i, zgot_ref, p_ref, o_ref, gain_ref, mix_ref)

    @pl.loop(0, 7)
    def _(s):
        near = lax.div(s, 2) + 1
        half0 = lax.rem(s, 2)
        for way in range(2):
            half = half0 if way == 0 else 1 - half0
            column = lax.rem(chip + (YN - near if way == 0 else near), YN) * 2 + 1 - core
            side(2 * s + way, column, half).wait_recv()

    for order in range(2):
        side(14 + order, partner, order).wait_recv()

    project(mix_ref, wall_ref, out_ref)

    @pl.loop(1, SP)
    def _(j):
        other = lax.rem(me + j, SP)
        send_message(other).wait_send()
        send_state(other).wait_send()

    @pl.loop(0, 7)
    def _(s):
        for way in range(2):
            ring(way, s, dp, 0).wait_send()
            side(2 * s + way, dp, 0).wait_send()

    for order in range(2):
        side(14 + order, dp, order).wait_send()


def per_device(query, key, value, decay_low, rate_low, decay_up, rate_up, base, gain, weight):
    vmem = pl.BlockSpec(memory_space=pltpu.VMEM)
    dma = pltpu.SemaphoreType.DMA
    out = pl.pallas_call(
        kernel,
        out_shape=jax.ShapeDtypeStruct((C, 2048), BF16),
        in_specs=[vmem] * 9 + [pl.BlockSpec(memory_space=pl.ANY)],
        out_specs=vmem,
        scratch_shapes=[
            pltpu.VMEM((C, C), BF16),
            pltpu.VMEM((SP, MSG, C), BF16),
            pltpu.VMEM((SP, MSG, C), BF16),
            pltpu.VMEM((4, 512, C), F32),
            pltpu.VMEM((SP, 32, C), BF16),
            pltpu.VMEM((SP, 32, C), BF16),
            pltpu.VMEM((PAIRS, C, 2 * C), BF16),
            pltpu.VMEM((PAIRS, C, C), F32),
            pltpu.VMEM((C, 2048), BF16),
            pltpu.VMEM((DPN, 2048, C), BF16),
            dma,
            dma((SP,)),
            dma((SP,)),
            dma((SP,)),
            dma((SP,)),
            dma((2, 7)),
            dma((2, 7)),
            dma((16,)),
            dma((16,)),
        ],
        compiler_params=pltpu.CompilerParams(
            collective_id=0, has_side_effects=True, vmem_limit_bytes=60 * 2**20
        ),
        name="mixer",
    )(
        query[0],
        key[0],
        value[0],
        decay_low[0],
        rate_low[0],
        decay_up,
        rate_up,
        base.reshape(PAIRS, C),
        gain.reshape(PAIRS, C),
        weight,
    )
    return out[None]


def solution(mesh):
    placed = (P("dp", "sp", None),) * 5 + (P(),) * 4 + (P(None, "dp"),)
    return jax.shard_map(
        per_device, mesh=mesh, in_specs=placed, out_specs=P("dp", "sp", None), check_vma=False
    )
```

```python
import jax
import jax.numpy as jnp
from jax import lax
from jax.experimental import pallas as pl
from jax.experimental.pallas import tpu as pltpu
from jax.sharding import PartitionSpec as P

F32 = jnp.float32
BF16 = jnp.bfloat16
C = 128
PAIRS = 16
SP = 32
DPN = 16
YN = 8
MSG = 80
DECAY_SCALE = 0.6065306597126334
MESH = pl.DeviceIdType.MESH


def split(x):
    high = x.astype(BF16)
    return high, (x - high.astype(F32)).astype(BF16)


def nn(a, b):
    return jnp.dot(a, b, preferred_element_type=F32)


def nt(a, b):
    return lax.dot_general(a, b, (((1,), (1,)), ((), ())), preferred_element_type=F32)


def rows_of(*parts):
    return jnp.concatenate(parts, axis=0)


def lanes_of(*parts):
    return jnp.concatenate(parts, axis=1)


def sigmoid(x):
    return 1.0 / (1.0 + jnp.exp(-x))


def iotas():
    return (
        lax.broadcasted_iota(jnp.int32, (C, C), 0),
        lax.broadcasted_iota(jnp.int32, (C, C), 1),
    )


def roll_half(x):
    return pltpu.roll(x, 64, 1)


def pair_front(pair, q_ref, k_ref, v_ref, sq_ref, rl_ref, du_ref, ru_ref, base_ref):
    row, col = iotas()
    first = col < 64
    at = pl.ds(pl.multiple_of(pair * C, C), C)
    decay_pre = (base_ref[pl.ds(pair, 1), :] + nn(sq_ref[...], du_ref[:, at])).astype(BF16).astype(F32)
    rate_pre = nn(rl_ref[...], ru_ref[:, at]).astype(BF16).astype(F32)
    log_decay = -DECAY_SCALE * sigmoid(decay_pre)
    rate = sigmoid(rate_pre)
    tri = jnp.where(row >= col, 1.0, 0.0).astype(BF16)
    ld_h, ld_l = split(log_decay)
    running = nn(lanes_of(tri, tri), rows_of(ld_h, ld_l))
    key = k_ref[:, at].astype(F32)
    query = q_ref[:, at].astype(F32)
    same = jnp.where((row < 64) == first, 1.0, 0.0).astype(BF16)
    sq_h, sq_l = split(key * key)
    unit = key * lax.rsqrt(1.0 + nn(lanes_of(sq_h, sq_l), rows_of(same, same)))
    erase = unit * rate
    centre = running[63:64, :]
    final = running[C - 1 : C, :]
    up = jnp.exp(running - centre)
    down = jnp.exp(centre - running)
    before = jnp.exp(running - log_decay - centre)
    from_start = jnp.exp(centre)
    to_end = jnp.exp(final - centre)
    f1 = unit * before
    f2 = query * up
    g1 = key * down
    g2 = erase * down
    return f1, f2, g1, g2, f1 * from_start, f2 * from_start, g1 * to_end, g2 * to_end, jnp.exp(final)


def invert_unit_lower(lows):
    row, col = iotas()
    differ = row ^ col
    zero = jnp.zeros((C, C), BF16)
    lane16 = lax.broadcasted_iota(jnp.int32, (16, C), 1)
    row16 = lax.broadcasted_iota(jnp.int32, (16, C), 0)
    inner = row16 ^ (lane16 & 15)

    def gather(low):
        out = low[0:16]
        for b in range(1, 8):
            out = jnp.where((lane16 >> 4) == b, low[16 * b : 16 * b + 16], out)
        return out

    def spread(small, size):
        own = (row // size) == (col // size)
        tiled = rows_of(*[small.astype(BF16)] * (C // size)) if size < C else small.astype(BF16)
        return jnp.where(own, tiled, zero)

    eye = jnp.where(inner == 0, 1.0, 0.0)
    small = [eye - jnp.where(inner == 1, gather(low).astype(F32), 0.0) for low in lows]
    size = 2
    while size < 16:
        level = (differ >= size) & (differ < 2 * size)
        mid = [nn(s.astype(BF16), jnp.where(level, low, zero)).astype(BF16) for s, low in zip(small, lows)]
        small = [s - nn(m, spread(s, 16)) for s, m in zip(small, mid)]
        size *= 2
    while size < C:
        level = (differ >= size) & (differ < 2 * size)
        even = (lax.broadcasted_iota(jnp.int32, (size, C), 1) & size) == 0
        mid = [
            nn(jnp.where(even, 0.0, s).astype(BF16), jnp.where(level, low, zero)).astype(BF16)
            for s, low in zip(small, lows)
        ]
        corner = [nn(m, spread(s, size)) for s, m in zip(small, mid)]
        small = [rows_of(jnp.where(even, s, 0.0), jnp.where(even, -c, s)) for s, c in zip(small, corner)]
        size *= 2
    return [s.astype(BF16) for s in small]


def group_body(pairs, refs, msg_ref, p_ref, o_ref):
    v_ref = refs[2]
    row, col = iotas()
    first = col < 64
    first_b = lax.broadcasted_iota(jnp.int32, (2 * C, C), 1) < 64
    strict = row > col
    within = row >= col
    zero2 = jnp.zeros((2 * C, C), BF16)
    zero1 = jnp.zeros((C, C), BF16)
    ep, kp, rk, re, ends, v_rolls = [], [], [], [], [], []
    for pair in pairs:
        at = pl.ds(pl.multiple_of(pair * C, C), C)
        f1, f2, g1, g2, es, qs, ke, ee, efin = pair_front(pair, *refs)
        ends.append((es, qs, ke, ee, efin))
        v_rolls.append(roll_half(v_ref[:, at].astype(F32)).astype(BF16))
        f_h, f_l = split(rows_of(f1, f2))
        g_h, g_l = split(rows_of(g1, g2))
        gg = lanes_of(g_h, g_h)
        for i in range(2):
            a_h = jnp.where(first_b, f_h, zero2) if i == 0 else jnp.where(first_b, zero2, f_h)
            a_l = jnp.where(first_b, f_l, zero2) if i == 0 else jnp.where(first_b, zero2, f_l)
            g = nt(lanes_of(a_h, a_l), gg) + nt(a_h, g_l)
            kp.append(split(jnp.where(strict, g[:C, :C], 0.0)))
            ep.append(split(jnp.where(strict, g[:C, C:], 0.0)))
            rk.append(split(jnp.where(within, g[C:, :C], 0.0)))
            re.append(split(jnp.where(within, g[C:, C:], 0.0)))
    heads = range(2 * len(pairs))
    carried = [nn(lanes_of(*kp[n]), rows_of(v_rolls[n // 2], v_rolls[n // 2])) for n in heads]
    xb = invert_unit_lower([e[0] for e in ep])
    rhs = [
        jnp.where(first, ends[n // 2][0], carried[n]) if n % 2 == 0 else jnp.where(first, carried[n], ends[n // 2][0])
        for n in heads
    ]
    s0 = [nn(xb[n], rhs[n].astype(BF16)).astype(BF16) for n in heads]
    resid = [rhs[n] - s0[n].astype(F32) - nn(lanes_of(*ep[n]), rows_of(s0[n], s0[n])) for n in heads]
    sol = [s0[n].astype(F32) + nn(xb[n], resid[n].astype(BF16)) for n in heads]
    outs = []
    for n in heads:
        _, _, ke, ee, _ = ends[n // 2]
        half = slice(64 * (n % 2), 64 * (n % 2) + 64)
        ee_h, ee_l = split(ee.T[half])
        ke_h, ke_l = split(ke.T[half])
        n_h, n_l = split(-sol[n])
        v_roll = v_rolls[n // 2]
        v_mine = jnp.where(first, zero1, v_roll) if n % 2 == 0 else jnp.where(first, v_roll, zero1)
        w_h = rows_of(n_h, v_mine)
        l_h = rows_of(lanes_of(ee_h, ke_h), lanes_of(re[n][0], rk[n][0]))
        l_l = rows_of(lanes_of(ee_l, ke_l), lanes_of(re[n][1], rk[n][1]))
        outs.append(nn(l_h, w_h) + nn(l_l, w_h) + nn(rows_of(ee_h, re[n][0]), n_l))
    low_rows = lax.broadcasted_iota(jnp.int32, (16, C), 0) < 8
    for m, pair in enumerate(pairs):
        d_h, d_l = split(jnp.broadcast_to(ends[m][4], (16, C)))
        d_tile = jnp.where(low_rows, d_h, d_l)
        for i in range(2):
            msg_ref[2 * pair + i, pl.ds(0, 64), :] = outs[2 * m + i][:64].astype(BF16)
            msg_ref[2 * pair + i, pl.ds(64, 16), :] = d_tile
        p_all = ends[m][1] + jnp.where(first, outs[2 * m][64:], outs[2 * m + 1][64:])
        o_all = roll_half(jnp.where(first, outs[2 * m + 1][64:], outs[2 * m][64:]))
        p_h, p_l = split(p_all)
        p_ref[pair] = lanes_of(p_h, p_l)
        o_ref[pair] = o_all


def compose_chunks(odd, msg_ref, zs_ref, g_ref):
    row = lax.broadcasted_iota(jnp.int32, (64, C), 0)
    col = lax.broadcasted_iota(jnp.int32, (64, C), 1)
    left = col < 64
    groups, per = 4, 8
    state = [jnp.where(row == col, 1.0, 0.0) for _ in range(groups)]
    zero = jnp.zeros((64, C), BF16)
    for step in range(per):
        for g in range(groups):
            c = g * per + step
            g_ref[g, pl.ds(64 * step, 64), :] = state[g]
            m = msg_ref[c, pl.ds(0, 64), :].astype(F32)
            tile = msg_ref[c, pl.ds(64, 16), :].astype(F32)
            d = tile[0:1, :] + tile[8:9, :]
            m = jnp.where(odd, roll_half(m), m)
            d = jnp.where(odd, roll_half(jnp.broadcast_to(d, (8, C)))[0:1, :], d)
            trans = jnp.where(left, m + jnp.where(row == col, d, 0.0), 0.0)
            add = jnp.where(left, 0.0, m)
            t_h, t_l = split(trans)
            lhs = lanes_of(jnp.where(left, t_h.astype(F32), roll_half(t_l.astype(F32))).astype(BF16), t_h)
            s_h, s_l = split(state[g])
            state[g] = nn(lhs, rows_of(s_h, s_h, s_l, zero)) + add
    starts = [None]
    z = jnp.where(left, roll_half(state[0]), 0.0)
    for g in range(1, groups):
        starts.append(z)
        if g < groups - 1:
            z = jnp.where(left, apply_state(state[g], z, left) + roll_half(state[g]), 0.0)
    for g in range(groups):
        stack = g_ref[g]
        wide = lax.broadcasted_iota(jnp.int32, (64 * per, C), 1) < 64
        total = roll_half(stack)
        if g > 0:
            total = total + apply_state(stack, starts[g], wide)
        for step in range(per):
            zc = total[64 * step : 64 * step + 64]
            packed = jnp.where(left[:32], zc[:32], roll_half(zc[32:]))
            zs_ref[g * per + step] = packed.astype(BF16)


def apply_state(stack, z, left):
    t_h, t_l = split(jnp.where(left, stack, 0.0))
    z_h, z_l = split(z)
    zero = jnp.zeros((64, C), BF16)
    lhs = lanes_of(jnp.where(left, t_h.astype(F32), roll_half(t_l.astype(F32))).astype(BF16), t_h)
    return nn(lhs, rows_of(z_h, z_h, z_l, zero))


GF = GROUP = 4


def group_finish(pairs, z_ref, p_ref, o_ref, gain_ref, mix_ref):
    row, col = iotas()
    left = lax.broadcasted_iota(jnp.int32, (32, C), 1) < 64
    mean_w = jnp.where((row < 64) == (col < 64), 1.0 / 64, 0.0).astype(BF16)
    mean_w = rows_of(mean_w, mean_w)
    reads = []
    for pair in pairs:
        za = z_ref[2 * pair].astype(F32)
        zb = z_ref[2 * pair + 1].astype(F32)
        zw = rows_of(
            jnp.where(left, za, 0.0),
            jnp.where(left, roll_half(za), 0.0),
            jnp.where(left, 0.0, roll_half(zb)),
            jnp.where(left, 0.0, zb),
        ).astype(BF16)
        reads.append(o_ref[pair] + nn(p_ref[pair], rows_of(zw, zw)))
    centred = [r - nn(lanes_of(*split(r)), mean_w) for r in reads]
    var = [nn(lanes_of(*split(c * c)), mean_w) for c in centred]
    for pair, c, v in zip(pairs, centred, var):
        at = pl.ds(pl.multiple_of(pair * C, C), C)
        mix_ref[:, at] = (c * lax.rsqrt(v + 1.0) * gain_ref[pl.ds(pair, 1), :]).astype(BF16)


def project(mix_ref, w_ref, out_ref):
    @pl.loop(0, YN)
    def _(y):
        acc = jnp.zeros((C, 2 * C), F32)
        for k in range(8):
            w = lanes_of(w_ref[2 * y, pl.ds(256 * k, 256), :], w_ref[2 * y + 1, pl.ds(256 * k, 256), :])
            acc = acc + nn(mix_ref[:, pl.ds(256 * k, 256)], w)
        out_ref[:, pl.ds(pl.multiple_of(y * 256, 256), 256)] = acc.astype(BF16)


def remote(src, dst, send, recv, **where):
    return pltpu.make_async_remote_copy(
        src_ref=src, dst_ref=dst, send_sem=send, recv_sem=recv, device_id=where, device_id_type=MESH
    )


def kernel(
    q_ref,
    k_ref,
    v_ref,
    dl_ref,
    rl_ref,
    du_ref,
    ru_ref,
    base_ref,
    gain_ref,
    w_ref,
    out_ref,
    sq_ref,
    msg_ref,
    got_ref,
    group_ref,
    zs_ref,
    zgot_ref,
    p_ref,
    o_ref,
    mix_ref,
    wall_ref,
    own_sem,
    msg_send,
    msg_recv,
    z_send,
    z_recv,
    ring_send,
    ring_recv,
    side_send,
    side_recv,
):
    me = lax.axis_index("sp")
    dp = lax.axis_index("dp")
    core = lax.rem(dp, 2)
    chip = lax.div(dp, 2)
    partner = dp + 1 - 2 * core
    up = lax.rem(dp + 2, DPN)
    down = lax.rem(dp + DPN - 2, DPN)

    barrier = pltpu.get_barrier_semaphore()

    @pl.loop(1, SP)
    def _(j):
        pl.semaphore_signal(
            barrier, inc=1, device_id={"sp": lax.rem(me + j, SP)}, device_id_type=MESH
        )

    for other in (partner, up, down):
        pl.semaphore_signal(barrier, inc=1, device_id={"dp": other}, device_id_type=MESH)
    own = pltpu.make_async_copy(w_ref, wall_ref.at[dp], own_sem)
    own.start()
    sq_ref[...] = jnp.tanh(dl_ref[...].astype(F32)).astype(BF16)
    own.wait()
    pl.semaphore_wait(barrier, SP + 2)

    def piece(column, half):
        return wall_ref.at[column, pl.ds(half * 1024, 1024), :]

    def ring(way, order, column, half):
        ref = piece(column, half)
        return remote(ref, ref, ring_send.at[way, order], ring_recv.at[way, order], dp=(up, down)[way])

    def side(slot, column, half):
        ref = piece(column, half)
        return remote(ref, ref, side_send.at[slot], side_recv.at[slot], dp=partner)

    for order in range(2):
        ring(0, order, dp, order).start()
        ring(1, order, dp, 1 - order).start()
        side(14 + order, dp, order).start()

    def ring_step(s):
        near = s // 2 + 1
        half0 = s % 2
        for way in range(2):
            half = half0 if way == 0 else 1 - half0
            column = lax.rem(chip + (YN - near if way == 0 else near), YN) * 2 + core
            ring(way, s, column, half).wait_recv()

            if not isinstance(s, int) or s < 5:
                ring(way, s + 2, column, half).start()

            side(2 * s + way, column, half).start()

    def send_message(head):
        return remote(
            msg_ref.at[head], got_ref.at[me], msg_send.at[head], msg_recv.at[me], sp=head
        )

    def send_pair(pair):
        for i in range(2):
            head = 2 * pair + i

            @pl.when(head != me)
            def _():
                send_message(head).start()

    first_pair = lax.div(me, 2)
    refs = (q_ref, k_ref, v_ref, sq_ref, rl_ref, du_ref, ru_ref, base_ref)

    def pairs_of(i):
        return [lax.rem(first_pair + GROUP * i + j, PAIRS) for j in range(GROUP)]

    def send_group(i):
        for pair in pairs_of(i):
            send_pair(pair)

    @pl.loop(0, PAIRS // GROUP)
    def _(i):
        @pl.when(i > 0)
        def _():
            send_group(i - 1)

        @pl.when(i >= 2)
        def _():
            ring_step(i - 2)

        group_body(pairs_of(i), refs, msg_ref, p_ref, o_ref)

    got_ref[me] = msg_ref[me]
    send_group(PAIRS // GROUP - 1)
    ring_step(2)

    @pl.loop(1, SP)
    def _(j):
        other = lax.rem(me + j, SP)
        remote(
            msg_ref.at[me], got_ref.at[other], msg_send.at[other], msg_recv.at[other], sp=other
        ).wait_recv()

    ring_step(3)
    compose_chunks(lax.rem(me, 2) == 1, got_ref, zs_ref, group_ref)

    def send_state(chunk):
        return remote(
            zs_ref.at[chunk], zgot_ref.at[me], z_send.at[chunk], z_recv.at[me], sp=chunk
        )

    zgot_ref[me] = zs_ref[me]

    @pl.loop(1, SP)
    def _(j):
        send_state(lax.rem(me + j, SP)).start()

    ring_step(4)

    @pl.loop(1, SP)
    def _(j):
        other = lax.rem(me + SP - j, SP)
        remote(
            zs_ref.at[me], zgot_ref.at[other], z_send.at[other], z_recv.at[other], sp=other
        ).wait_recv()

    @pl.loop(0, PAIRS // GROUP)
    def _(i):
        group_finish([GROUP * i + j for j in range(GROUP)], zgot_ref, p_ref, o_ref, gain_ref, mix_ref)

    ring_step(5)
    ring_step(6)

    @pl.loop(0, 7)
    def _(s):
        near = lax.div(s, 2) + 1
        half0 = lax.rem(s, 2)
        for way in range(2):
            half = half0 if way == 0 else 1 - half0
            column = lax.rem(chip + (YN - near if way == 0 else near), YN) * 2 + 1 - core
            side(2 * s + way, column, half).wait_recv()

    for order in range(2):
        side(14 + order, partner, order).wait_recv()

    project(mix_ref, wall_ref, out_ref)

    @pl.loop(1, SP)
    def _(j):
        other = lax.rem(me + j, SP)
        send_message(other).wait_send()
        send_state(other).wait_send()

    @pl.loop(0, 7)
    def _(s):
        for way in range(2):
            ring(way, s, dp, 0).wait_send()
            side(2 * s + way, dp, 0).wait_send()

    for order in range(2):
        side(14 + order, dp, order).wait_send()


def per_device(query, key, value, decay_low, rate_low, decay_up, rate_up, base, gain, weight):
    vmem = pl.BlockSpec(memory_space=pltpu.VMEM)
    dma = pltpu.SemaphoreType.DMA
    out = pl.pallas_call(
        kernel,
        out_shape=jax.ShapeDtypeStruct((C, 2048), BF16),
        in_specs=[vmem] * 9 + [pl.BlockSpec(memory_space=pl.ANY)],
        out_specs=vmem,
        scratch_shapes=[
            pltpu.VMEM((C, C), BF16),
            pltpu.VMEM((SP, MSG, C), BF16),
            pltpu.VMEM((SP, MSG, C), BF16),
            pltpu.VMEM((4, 512, C), F32),
            pltpu.VMEM((SP, 32, C), BF16),
            pltpu.VMEM((SP, 32, C), BF16),
            pltpu.VMEM((PAIRS, C, 2 * C), BF16),
            pltpu.VMEM((PAIRS, C, C), F32),
            pltpu.VMEM((C, 2048), BF16),
            pltpu.VMEM((DPN, 2048, C), BF16),
            dma,
            dma((SP,)),
            dma((SP,)),
            dma((SP,)),
            dma((SP,)),
            dma((2, 7)),
            dma((2, 7)),
            dma((16,)),
            dma((16,)),
        ],
        compiler_params=pltpu.CompilerParams(
            collective_id=0, has_side_effects=True, vmem_limit_bytes=60 * 2**20
        ),
        name="mixer",
    )(
        query[0],
        key[0],
        value[0],
        decay_low[0],
        rate_low[0],
        decay_up,
        rate_up,
        base.reshape(PAIRS, C),
        gain.reshape(PAIRS, C),
        weight,
    )
    return out[None]


def solution(mesh):
    placed = (P("dp", "sp", None),) * 5 + (P(),) * 4 + (P(None, "dp"),)
    return jax.shard_map(
        per_device, mesh=mesh, in_specs=placed, out_specs=P("dp", "sp", None), check_vma=False
    )
```

```python
import jax
import jax.numpy as jnp
from jax import lax
from jax.experimental import pallas as pl
from jax.experimental.pallas import tpu as pltpu
from jax.sharding import PartitionSpec as P

F32 = jnp.float32
BF16 = jnp.bfloat16
C = 128
PAIRS = 16
SP = 32
DPN = 16
YN = 8
MSG = 80
DECAY_SCALE = 0.6065306597126334
MESH = pl.DeviceIdType.MESH


def split(x):
    high = x.astype(BF16)
    return high, (x - high.astype(F32)).astype(BF16)


def nn(a, b):
    return jnp.dot(a, b, preferred_element_type=F32)


def nt(a, b):
    return lax.dot_general(a, b, (((1,), (1,)), ((), ())), preferred_element_type=F32)


def rows_of(*parts):
    return jnp.concatenate(parts, axis=0)


def lanes_of(*parts):
    return jnp.concatenate(parts, axis=1)


def sigmoid(x):
    return 1.0 / (1.0 + jnp.exp(-x))


def iotas():
    return (
        lax.broadcasted_iota(jnp.int32, (C, C), 0),
        lax.broadcasted_iota(jnp.int32, (C, C), 1),
    )


def roll_half(x):
    return pltpu.roll(x, 64, 1)


def pair_front(pair, q_ref, k_ref, v_ref, sq_ref, rl_ref, du_ref, ru_ref, base_ref):
    row, col = iotas()
    first = col < 64
    at = pl.ds(pl.multiple_of(pair * C, C), C)
    decay_pre = (base_ref[pl.ds(pair, 1), :] + nn(sq_ref[...], du_ref[:, at])).astype(BF16).astype(F32)
    rate_pre = nn(rl_ref[...], ru_ref[:, at]).astype(BF16).astype(F32)
    log_decay = -DECAY_SCALE * sigmoid(decay_pre)
    rate = sigmoid(rate_pre)
    tri = jnp.where(row >= col, 1.0, 0.0).astype(BF16)
    ld_h, ld_l = split(log_decay)
    running = nn(lanes_of(tri, tri), rows_of(ld_h, ld_l))
    key = k_ref[:, at].astype(F32)
    query = q_ref[:, at].astype(F32)
    same = jnp.where((row < 64) == first, 1.0, 0.0).astype(BF16)
    sq_h, sq_l = split(key * key)
    unit = key * lax.rsqrt(1.0 + nn(lanes_of(sq_h, sq_l), rows_of(same, same)))
    erase = unit * rate
    centre = running[63:64, :]
    final = running[C - 1 : C, :]
    up = jnp.exp(running - centre)
    down = jnp.exp(centre - running)
    before = jnp.exp(running - log_decay - centre)
    from_start = jnp.exp(centre)
    to_end = jnp.exp(final - centre)
    f1 = unit * before
    f2 = query * up
    g1 = key * down
    g2 = erase * down
    return f1, f2, g1, g2, f1 * from_start, f2 * from_start, g1 * to_end, g2 * to_end, jnp.exp(final)


def invert_unit_lower(lows):
    row, col = iotas()
    differ = row ^ col
    zero = jnp.zeros((C, C), BF16)
    lane16 = lax.broadcasted_iota(jnp.int32, (16, C), 1)
    row16 = lax.broadcasted_iota(jnp.int32, (16, C), 0)
    inner = row16 ^ (lane16 & 15)

    def gather(low):
        out = low[0:16]
        for b in range(1, 8):
            out = jnp.where((lane16 >> 4) == b, low[16 * b : 16 * b + 16], out)
        return out

    def spread(small, size):
        own = (row // size) == (col // size)
        tiled = rows_of(*[small.astype(BF16)] * (C // size)) if size < C else small.astype(BF16)
        return jnp.where(own, tiled, zero)

    eye = jnp.where(inner == 0, 1.0, 0.0)
    wide_row = lax.broadcasted_iota(jnp.int32, (C, 16 * C), 0)
    wide_col = lax.broadcasted_iota(jnp.int32, (C, 16 * C), 1)
    pick = (wide_row & 15) == (wide_col // C)
    pick = jnp.where(pick & ((wide_row >> 4) == ((wide_col % C) >> 4)), 1.0, 0.0).astype(BF16)
    packed = [gather(low) for low in lows]
    columns = nn(rows_of(*packed), pick)
    small = []
    for n in range(len(lows)):
        x = eye
        for s in range(15):
            x = x - columns[16 * n : 16 * n + 16, C * s : C * s + C] * x[s : s + 1]
        small.append(x)
    size = 16
    while size < C:
        level = (differ >= size) & (differ < 2 * size)
        even = (lax.broadcasted_iota(jnp.int32, (size, C), 1) & size) == 0
        mid = [
            nn(jnp.where(even, 0.0, s).astype(BF16), jnp.where(level, low, zero)).astype(BF16)
            for s, low in zip(small, lows)
        ]
        corner = [nn(m, spread(s, size)) for s, m in zip(small, mid)]
        small = [rows_of(jnp.where(even, s, 0.0), jnp.where(even, -c, s)) for s, c in zip(small, corner)]
        size *= 2
    return [s.astype(BF16) for s in small]


def masked(x, i):
    first = lax.broadcasted_iota(jnp.int32, x.shape, 1) < 64
    zero = jnp.zeros(x.shape, x.dtype)
    return jnp.where(first, x, zero) if i == 0 else jnp.where(first, zero, x)


def group_states(pairs, refs, msg_ref, hold):
    f_ref, g_ref, qs_ref, w_ref, n_ref = hold
    v_ref = refs[2]
    row, col = iotas()
    first = col < 64
    strict = row > col
    ep, kp, ends, v_rolls = [], [], [], []
    for pair in pairs:
        at = pl.ds(pl.multiple_of(pair * C, C), C)
        f1, f2, g1, g2, es, qs, ke, ee, efin = pair_front(pair, *refs)
        qs_ref[pair] = qs
        f_ref[pair] = lanes_of(*split(f2))
        ends.append((es, ke, ee, efin))
        v_rolls.append(roll_half(v_ref[:, at].astype(F32)).astype(BF16))
        f_h, f_l = split(f1)
        g_h, g_l = split(rows_of(g1, g2))
        g_ref[pair] = lanes_of(g_h, g_l)
        gg = lanes_of(g_h, g_h)
        for i in range(2):
            a_h, a_l = masked(f_h, i), masked(f_l, i)
            g = nt(lanes_of(a_h, a_l), gg) + nt(a_h, g_l)
            kp.append(split(jnp.where(strict, g[:, :C], 0.0)))
            ep.append(split(jnp.where(strict, g[:, C:], 0.0)))
    heads = range(2 * len(pairs))
    carried = [nn(lanes_of(*kp[n]), rows_of(v_rolls[n // 2], v_rolls[n // 2])) for n in heads]
    xb = invert_unit_lower([e[0] for e in ep])
    rhs = [
        jnp.where(first, ends[n // 2][0], carried[n]) if n % 2 == 0 else jnp.where(first, carried[n], ends[n // 2][0])
        for n in heads
    ]
    s0 = [nn(xb[n], rhs[n].astype(BF16)).astype(BF16) for n in heads]
    resid = [rhs[n] - s0[n].astype(F32) - nn(lanes_of(*ep[n]), rows_of(s0[n], s0[n])) for n in heads]
    sol = [s0[n].astype(F32) + nn(xb[n], resid[n].astype(BF16)) for n in heads]
    low_rows = lax.broadcasted_iota(jnp.int32, (16, C), 0) < 8
    for n in heads:
        _, ke, ee, efin = ends[n // 2]
        head = 2 * pairs[n // 2] + n % 2
        half = slice(64 * (n % 2), 64 * (n % 2) + 64)
        ee_h, ee_l = split(ee.T[half])
        ke_h, ke_l = split(ke.T[half])
        n_h, n_l = split(-sol[n])
        w_h = rows_of(n_h, masked(v_rolls[n // 2], 1 - n % 2))
        w_ref[head] = w_h
        n_ref[head] = n_l
        out = nn(lanes_of(ee_h, ke_h), w_h) + nn(lanes_of(ee_l, ke_l), w_h) + nn(ee_h, n_l)
        d_h, d_l = split(jnp.broadcast_to(efin, (16, C)))
        msg_ref[head, pl.ds(0, 64), :] = out.astype(BF16)
        msg_ref[head, pl.ds(64, 16), :] = jnp.where(low_rows, d_h, d_l)


def group_reads(pairs, hold, p_ref, o_ref):
    f_ref, g_ref, qs_ref, w_ref, n_ref = hold
    row, col = iotas()
    first = col < 64
    within = row >= col
    for pair in pairs:
        g_h, g_l = g_ref[pair, :, pl.ds(0, C)], g_ref[pair, :, pl.ds(C, C)]
        gg = lanes_of(g_h, g_h)
        f_h, f_l = f_ref[pair, :, pl.ds(0, C)], f_ref[pair, :, pl.ds(C, C)]
        outs = []
        for i in range(2):
            a_h, a_l = masked(f_h, i), masked(f_l, i)
            g = nt(lanes_of(a_h, a_l), gg) + nt(a_h, g_l)
            rk_h, rk_l = split(jnp.where(within, g[:, :C], 0.0))
            re_h, re_l = split(jnp.where(within, g[:, C:], 0.0))
            w_h = w_ref[2 * pair + i]
            outs.append(nn(lanes_of(re_h, rk_h), w_h) + nn(lanes_of(re_l, rk_l), w_h) + nn(re_h, n_ref[2 * pair + i]))
        p_ref[pair] = lanes_of(*split(qs_ref[pair] + jnp.where(first, outs[0], outs[1])))
        o_ref[pair] = roll_half(jnp.where(first, outs[1], outs[0]))


def compose_chunks(odd, msg_ref, zs_ref, g_ref):
    row = lax.broadcasted_iota(jnp.int32, (64, C), 0)
    col = lax.broadcasted_iota(jnp.int32, (64, C), 1)
    left = col < 64
    groups, per = 4, 8
    state = [jnp.where(row == col, 1.0, 0.0) for _ in range(groups)]
    zero = jnp.zeros((64, C), BF16)
    for step in range(per):
        for g in range(groups):
            c = g * per + step
            g_ref[g, pl.ds(64 * step, 64), :] = state[g]
            m = msg_ref[c, pl.ds(0, 64), :].astype(F32)
            tile = msg_ref[c, pl.ds(64, 16), :].astype(F32)
            d = tile[0:1, :] + tile[8:9, :]
            m = jnp.where(odd, roll_half(m), m)
            d = jnp.where(odd, roll_half(jnp.broadcast_to(d, (8, C)))[0:1, :], d)
            trans = jnp.where(left, m + jnp.where(row == col, d, 0.0), 0.0)
            add = jnp.where(left, 0.0, m)
            t_h, t_l = split(trans)
            lhs = lanes_of(jnp.where(left, t_h.astype(F32), roll_half(t_l.astype(F32))).astype(BF16), t_h)
            s_h, s_l = split(state[g])
            state[g] = nn(lhs, rows_of(s_h, s_h, s_l, zero)) + add
    starts = [None]
    z = jnp.where(left, roll_half(state[0]), 0.0)
    for g in range(1, groups):
        starts.append(z)
        if g < groups - 1:
            z = jnp.where(left, apply_state(state[g], z, left) + roll_half(state[g]), 0.0)
    for g in range(groups):
        stack = g_ref[g]
        wide = lax.broadcasted_iota(jnp.int32, (64 * per, C), 1) < 64
        total = roll_half(stack)
        if g > 0:
            total = total + apply_state(stack, starts[g], wide)
        for step in range(per):
            zc = total[64 * step : 64 * step + 64]
            packed = jnp.where(left[:32], zc[:32], roll_half(zc[32:]))
            zs_ref[g * per + step] = packed.astype(BF16)


def apply_state(stack, z, left):
    t_h, t_l = split(jnp.where(left, stack, 0.0))
    z_h, z_l = split(z)
    zero = jnp.zeros((64, C), BF16)
    lhs = lanes_of(jnp.where(left, t_h.astype(F32), roll_half(t_l.astype(F32))).astype(BF16), t_h)
    return nn(lhs, rows_of(z_h, z_h, z_l, zero))


GF = GROUP = 4


def group_finish(pairs, z_ref, p_ref, o_ref, gain_ref, mix_ref):
    row, col = iotas()
    left = lax.broadcasted_iota(jnp.int32, (32, C), 1) < 64
    mean_w = jnp.where((row < 64) == (col < 64), 1.0 / 64, 0.0).astype(BF16)
    mean_w = rows_of(mean_w, mean_w)
    reads = []
    for pair in pairs:
        za = z_ref[2 * pair].astype(F32)
        zb = z_ref[2 * pair + 1].astype(F32)
        zw = rows_of(
            jnp.where(left, za, 0.0),
            jnp.where(left, roll_half(za), 0.0),
            jnp.where(left, 0.0, roll_half(zb)),
            jnp.where(left, 0.0, zb),
        ).astype(BF16)
        reads.append(o_ref[pair] + nn(p_ref[pair], rows_of(zw, zw)))
    centred = [r - nn(lanes_of(*split(r)), mean_w) for r in reads]
    var = [nn(lanes_of(*split(c * c)), mean_w) for c in centred]
    for pair, c, v in zip(pairs, centred, var):
        at = pl.ds(pl.multiple_of(pair * C, C), C)
        mix_ref[:, at] = (c * lax.rsqrt(v + 1.0) * gain_ref[pl.ds(pair, 1), :]).astype(BF16)


def project(mix_ref, w_ref, out_ref):
    @pl.loop(0, YN)
    def _(y):
        acc = jnp.zeros((C, 2 * C), F32)
        for k in range(8):
            w = lanes_of(w_ref[2 * y, pl.ds(256 * k, 256), :], w_ref[2 * y + 1, pl.ds(256 * k, 256), :])
            acc = acc + nn(mix_ref[:, pl.ds(256 * k, 256)], w)
        out_ref[:, pl.ds(pl.multiple_of(y * 256, 256), 256)] = acc.astype(BF16)


def remote(src, dst, send, recv, **where):
    return pltpu.make_async_remote_copy(
        src_ref=src, dst_ref=dst, send_sem=send, recv_sem=recv, device_id=where, device_id_type=MESH
    )


def kernel(
    q_ref,
    k_ref,
    v_ref,
    dl_ref,
    rl_ref,
    du_ref,
    ru_ref,
    base_ref,
    gain_ref,
    weight_ref,
    out_ref,
    sq_ref,
    msg_ref,
    got_ref,
    group_ref,
    zs_ref,
    zgot_ref,
    p_ref,
    o_ref,
    mix_ref,
    wall_ref,
    f_ref,
    g_ref,
    qs_ref,
    w_ref,
    n_ref,
    own_sem,
    msg_send,
    msg_recv,
    z_send,
    z_recv,
    ring_send,
    ring_recv,
    side_send,
    side_recv,
):
    me = lax.axis_index("sp")
    dp = lax.axis_index("dp")
    core = lax.rem(dp, 2)
    chip = lax.div(dp, 2)
    partner = dp + 1 - 2 * core
    up = lax.rem(dp + 2, DPN)
    down = lax.rem(dp + DPN - 2, DPN)

    barrier = pltpu.get_barrier_semaphore()

    @pl.loop(1, SP)
    def _(j):
        pl.semaphore_signal(
            barrier, inc=1, device_id={"sp": lax.rem(me + j, SP)}, device_id_type=MESH
        )

    for other in (partner, up, down):
        pl.semaphore_signal(barrier, inc=1, device_id={"dp": other}, device_id_type=MESH)
    own = pltpu.make_async_copy(weight_ref, wall_ref.at[dp], own_sem)
    own.start()
    sq_ref[...] = jnp.tanh(dl_ref[...].astype(F32)).astype(BF16)
    with jax.named_scope('entry'):
        own.wait()
        pl.semaphore_wait(barrier, SP + 2)

    def piece(column, half):
        return wall_ref.at[column, pl.ds(half * 1024, 1024), :]

    def ring(way, order, column, half):
        ref = piece(column, half)
        return remote(ref, ref, ring_send.at[way, order], ring_recv.at[way, order], dp=(up, down)[way])

    def side(slot, column, half):
        ref = piece(column, half)
        return remote(ref, ref, side_send.at[slot], side_recv.at[slot], dp=partner)

    for order in range(2):
        ring(0, order, dp, order).start()
        ring(1, order, dp, 1 - order).start()
        side(14 + order, dp, order).start()

    def ring_step(s):
        near = s // 2 + 1
        half0 = s % 2
        for way in range(2):
            half = half0 if way == 0 else 1 - half0
            column = lax.rem(chip + (YN - near if way == 0 else near), YN) * 2 + core
            ring(way, s, column, half).wait_recv()

            if not isinstance(s, int) or s < 5:
                ring(way, s + 2, column, half).start()

            side(2 * s + way, column, half).start()

    def send_message(head):
        return remote(
            msg_ref.at[head], got_ref.at[me], msg_send.at[head], msg_recv.at[me], sp=head
        )

    def send_pair(pair):
        for i in range(2):
            head = 2 * pair + i

            @pl.when(head != me)
            def _():
                send_message(head).start()

    first_pair = lax.div(me, 2)
    hold = (f_ref, g_ref, qs_ref, w_ref, n_ref)
    refs = (q_ref, k_ref, v_ref, sq_ref, rl_ref, du_ref, ru_ref, base_ref)

    def pairs_of(i):
        return [lax.rem(first_pair + o, PAIRS) for o in (8 - 2 * i, 9 + 2 * i, 7 - 2 * i, 10 + 2 * i)]

    def send_group(i):
        for pair in pairs_of(i):
            send_pair(pair)

    @pl.loop(0, PAIRS // GROUP)
    def _(i):
        @pl.when(i > 0)
        def _():
            send_group(i - 1)

        with jax.named_scope('ringA'):
          @pl.when(i >= 2)
          def _():
            ring_step(i - 2)

        with jax.named_scope('group'):
            group_states(pairs_of(i), refs, msg_ref, hold)

    got_ref[me] = msg_ref[me]
    send_group(PAIRS // GROUP - 1)
    with jax.named_scope("ring2"):
        ring_step(2)

    def reads(i):
        with jax.named_scope("reads"):
            group_reads([GROUP * i + j for j in range(GROUP)], hold, p_ref, o_ref)

    pl.loop(0, 2)(reads)

    with jax.named_scope('msgwait'):
     @pl.loop(1, SP)
     def _(j):
        other = lax.rem(me + j, SP)
        remote(
            msg_ref.at[me], got_ref.at[other], msg_send.at[other], msg_recv.at[other], sp=other
        ).wait_recv()

    with jax.named_scope("ring3"):
        ring_step(3)
    with jax.named_scope('scan'):
        compose_chunks(lax.rem(me, 2) == 1, got_ref, zs_ref, group_ref)

    def send_state(chunk):
        return remote(
            zs_ref.at[chunk], zgot_ref.at[me], z_send.at[chunk], z_recv.at[me], sp=chunk
        )

    zgot_ref[me] = zs_ref[me]

    @pl.loop(1, SP)
    def _(j):
        send_state(lax.rem(me + j, SP)).start()

    with jax.named_scope("ring4"):
        ring_step(4)

    pl.loop(2, PAIRS // GROUP)(reads)

    with jax.named_scope('zwait'):
     @pl.loop(1, SP)
     def _(j):
        other = lax.rem(me + SP - j, SP)
        remote(
            zs_ref.at[me], zgot_ref.at[other], z_send.at[other], z_recv.at[other], sp=other
        ).wait_recv()

    with jax.named_scope('finish'):
     @pl.loop(0, PAIRS // GROUP)
     def _(i):
        group_finish([GROUP * i + j for j in range(GROUP)], zgot_ref, p_ref, o_ref, gain_ref, mix_ref)

    with jax.named_scope("ring5"):
        ring_step(5)
    with jax.named_scope("ring6"):
        ring_step(6)

    with jax.named_scope('sidewait'):
     @pl.loop(0, 7)
     def _(s):
        near = lax.div(s, 2) + 1
        half0 = lax.rem(s, 2)
        for way in range(2):
            half = half0 if way == 0 else 1 - half0
            column = lax.rem(chip + (YN - near if way == 0 else near), YN) * 2 + 1 - core
            side(2 * s + way, column, half).wait_recv()

    for order in range(2):
        side(14 + order, partner, order).wait_recv()

    with jax.named_scope('project'):
        project(mix_ref, wall_ref, out_ref)

    with jax.named_scope('tail'):
     @pl.loop(1, SP)
     def _(j):
        other = lax.rem(me + j, SP)
        send_message(other).wait_send()
        send_state(other).wait_send()

    @pl.loop(0, 7)
    def _(s):
        for way in range(2):
            ring(way, s, dp, 0).wait_send()
            side(2 * s + way, dp, 0).wait_send()

    for order in range(2):
        side(14 + order, dp, order).wait_send()


def per_device(query, key, value, decay_low, rate_low, decay_up, rate_up, base, gain, weight):
    vmem = pl.BlockSpec(memory_space=pltpu.VMEM)
    dma = pltpu.SemaphoreType.DMA
    out = pl.pallas_call(
        kernel,
        out_shape=jax.ShapeDtypeStruct((C, 2048), BF16),
        in_specs=[vmem] * 9 + [pl.BlockSpec(memory_space=pl.ANY)],
        out_specs=vmem,
        scratch_shapes=[
            pltpu.VMEM((C, C), BF16),
            pltpu.VMEM((SP, MSG, C), BF16),
            pltpu.VMEM((SP, MSG, C), BF16),
            pltpu.VMEM((4, 512, C), F32),
            pltpu.VMEM((SP, 32, C), BF16),
            pltpu.VMEM((SP, 32, C), BF16),
            pltpu.VMEM((PAIRS, C, 2 * C), BF16),
            pltpu.VMEM((PAIRS, C, C), F32),
            pltpu.VMEM((C, 2048), BF16),
            pltpu.VMEM((DPN, 2048, C), BF16),
            pltpu.VMEM((PAIRS, C, 2 * C), BF16),
            pltpu.VMEM((PAIRS, 2 * C, 2 * C), BF16),
            pltpu.VMEM((PAIRS, C, C), F32),
            pltpu.VMEM((SP, 2 * C, C), BF16),
            pltpu.VMEM((SP, C, C), BF16),
            dma,
            dma((SP,)),
            dma((SP,)),
            dma((SP,)),
            dma((SP,)),
            dma((2, 7)),
            dma((2, 7)),
            dma((16,)),
            dma((16,)),
        ],
        compiler_params=pltpu.CompilerParams(
            collective_id=0, has_side_effects=True, vmem_limit_bytes=60 * 2**20
        ),
        name="mixer",
    )(
        query[0],
        key[0],
        value[0],
        decay_low[0],
        rate_low[0],
        decay_up,
        rate_up,
        base.reshape(PAIRS, C),
        gain.reshape(PAIRS, C),
        weight,
    )
    return out[None]


def solution(mesh):
    placed = (P("dp", "sp", None),) * 5 + (P(),) * 4 + (P(None, "dp"),)
    return jax.shard_map(
        per_device, mesh=mesh, in_specs=placed, out_specs=P("dp", "sp", None), check_vma=False
    )
```

```python
import jax
import jax.numpy as jnp
from jax import lax
from jax.experimental import pallas as pl
from jax.experimental.pallas import tpu as pltpu
from jax.sharding import PartitionSpec as P

F32 = jnp.float32
BF16 = jnp.bfloat16
C = 128
PAIRS = 16
SP = 32
DPN = 16
YN = 8
MSG = 80
WHOLE = 1536
QUARTER = (2048 - WHOLE) // 4
DECAY_SCALE = 0.6065306597126334
MESH = pl.DeviceIdType.MESH


def split(x):
    high = x.astype(BF16)
    return high, (x - high.astype(F32)).astype(BF16)


def nn(a, b):
    return jnp.dot(a, b, preferred_element_type=F32)


def nt(a, b):
    return lax.dot_general(a, b, (((1,), (1,)), ((), ())), preferred_element_type=F32)


def rows_of(*parts):
    return jnp.concatenate(parts, axis=0)


def lanes_of(*parts):
    return jnp.concatenate(parts, axis=1)


def sigmoid(x):
    return 1.0 / (1.0 + jnp.exp(-x))


def iotas():
    return (
        lax.broadcasted_iota(jnp.int32, (C, C), 0),
        lax.broadcasted_iota(jnp.int32, (C, C), 1),
    )


def roll_half(x):
    return pltpu.roll(x, 64, 1)


def pair_front(pair, q_ref, k_ref, v_ref, sq_ref, rl_ref, du_ref, ru_ref, base_ref):
    row, col = iotas()
    first = col < 64
    at = pl.ds(pl.multiple_of(pair * C, C), C)
    decay_pre = (base_ref[pl.ds(pair, 1), :] + nn(sq_ref[...], du_ref[:, at])).astype(BF16).astype(F32)
    rate_pre = nn(rl_ref[...], ru_ref[:, at]).astype(BF16).astype(F32)
    log_decay = -DECAY_SCALE * sigmoid(decay_pre)
    rate = sigmoid(rate_pre)
    tri = jnp.where(row >= col, 1.0, 0.0).astype(BF16)
    ld_h, ld_l = split(log_decay)
    running = nn(lanes_of(tri, tri), rows_of(ld_h, ld_l))
    key = k_ref[:, at].astype(F32)
    query = q_ref[:, at].astype(F32)
    same = jnp.where((row < 64) == first, 1.0, 0.0).astype(BF16)
    sq_h, sq_l = split(key * key)
    unit = key * lax.rsqrt(1.0 + nn(lanes_of(sq_h, sq_l), rows_of(same, same)))
    erase = unit * rate
    centre = running[63:64, :]
    final = running[C - 1 : C, :]
    up = jnp.exp(running - centre)
    down = jnp.exp(centre - running)
    before = jnp.exp(running - log_decay - centre)
    from_start = jnp.exp(centre)
    to_end = jnp.exp(final - centre)
    f1 = unit * before
    f2 = query * up
    g1 = key * down
    g2 = erase * down
    return f1, f2, g1, g2, f1 * from_start, f2 * from_start, g1 * to_end, g2 * to_end, jnp.exp(final)


def invert_unit_lower(lows):
    row, col = iotas()
    differ = row ^ col
    zero = jnp.zeros((C, C), BF16)
    lane16 = lax.broadcasted_iota(jnp.int32, (16, C), 1)
    row16 = lax.broadcasted_iota(jnp.int32, (16, C), 0)
    inner = row16 ^ (lane16 & 15)

    def gather(low):
        out = low[0:16]
        for b in range(1, 8):
            out = jnp.where((lane16 >> 4) == b, low[16 * b : 16 * b + 16], out)
        return out

    def spread(small, size):
        own = (row // size) == (col // size)
        tiled = rows_of(*[small.astype(BF16)] * (C // size)) if size < C else small.astype(BF16)
        return jnp.where(own, tiled, zero)

    eye = jnp.where(inner == 0, 1.0, 0.0)
    wide_row = lax.broadcasted_iota(jnp.int32, (C, 16 * C), 0)
    wide_col = lax.broadcasted_iota(jnp.int32, (C, 16 * C), 1)
    pick = (wide_row & 15) == (wide_col // C)
    pick = jnp.where(pick & ((wide_row >> 4) == ((wide_col % C) >> 4)), 1.0, 0.0).astype(BF16)
    packed = [gather(low) for low in lows]
    columns = nn(rows_of(*packed), pick)
    small = []
    for n in range(len(lows)):
        x = eye
        for s in range(15):
            x = x - columns[16 * n : 16 * n + 16, C * s : C * s + C] * x[s : s + 1]
        small.append(x)
    size = 16
    while size < C:
        level = (differ >= size) & (differ < 2 * size)
        even = (lax.broadcasted_iota(jnp.int32, (size, C), 1) & size) == 0
        mid = [
            nn(jnp.where(even, 0.0, s).astype(BF16), jnp.where(level, low, zero)).astype(BF16)
            for s, low in zip(small, lows)
        ]
        corner = [nn(m, spread(s, size)) for s, m in zip(small, mid)]
        small = [rows_of(jnp.where(even, s, 0.0), jnp.where(even, -c, s)) for s, c in zip(small, corner)]
        size *= 2
    return [s.astype(BF16) for s in small]


def masked(x, i):
    first = lax.broadcasted_iota(jnp.int32, x.shape, 1) < 64
    zero = jnp.zeros(x.shape, x.dtype)
    return jnp.where(first, x, zero) if i == 0 else jnp.where(first, zero, x)


def group_states(pairs, refs, msg_ref, hold):
    f_ref, g_ref, qs_ref, w_ref, n_ref = hold
    v_ref = refs[2]
    row, col = iotas()
    first = col < 64
    strict = row > col
    ep, kp, ends, v_rolls = [], [], [], []
    for pair in pairs:
        at = pl.ds(pl.multiple_of(pair * C, C), C)
        f1, f2, g1, g2, es, qs, ke, ee, efin = pair_front(pair, *refs)
        qs_ref[pair] = qs
        f_ref[pair] = lanes_of(*split(f2))
        ends.append((es, ke, ee, efin))
        v_rolls.append(roll_half(v_ref[:, at].astype(F32)).astype(BF16))
        f_h, f_l = split(f1)
        g_h, g_l = split(rows_of(g1, g2))
        g_ref[pair] = lanes_of(g_h, g_l)
        gg = lanes_of(g_h, g_h)
        for i in range(2):
            a_h, a_l = masked(f_h, i), masked(f_l, i)
            g = nt(lanes_of(a_h, a_l), gg) + nt(a_h, g_l)
            kp.append(split(jnp.where(strict, g[:, :C], 0.0)))
            ep.append(split(jnp.where(strict, g[:, C:], 0.0)))
    heads = range(2 * len(pairs))
    carried = [nn(lanes_of(*kp[n]), rows_of(v_rolls[n // 2], v_rolls[n // 2])) for n in heads]
    xb = invert_unit_lower([e[0] for e in ep])
    rhs = [
        jnp.where(first, ends[n // 2][0], carried[n]) if n % 2 == 0 else jnp.where(first, carried[n], ends[n // 2][0])
        for n in heads
    ]
    s0 = [nn(xb[n], rhs[n].astype(BF16)).astype(BF16) for n in heads]
    resid = [rhs[n] - s0[n].astype(F32) - nn(lanes_of(*ep[n]), rows_of(s0[n], s0[n])) for n in heads]
    sol = [s0[n].astype(F32) + nn(xb[n], resid[n].astype(BF16)) for n in heads]
    low_rows = lax.broadcasted_iota(jnp.int32, (16, C), 0) < 8
    for n in heads:
        _, ke, ee, efin = ends[n // 2]
        head = 2 * pairs[n // 2] + n % 2
        half = slice(64 * (n % 2), 64 * (n % 2) + 64)
        ee_h, ee_l = split(ee.T[half])
        ke_h, ke_l = split(ke.T[half])
        n_h, n_l = split(-sol[n])
        w_h = rows_of(n_h, masked(v_rolls[n // 2], 1 - n % 2))
        w_ref[head] = w_h
        n_ref[head] = n_l
        out = nn(lanes_of(ee_h, ke_h), w_h) + nn(lanes_of(ee_l, ke_l), w_h) + nn(ee_h, n_l)
        d_h, d_l = split(jnp.broadcast_to(efin, (16, C)))
        msg_ref[head, pl.ds(0, 64), :] = out.astype(BF16)
        msg_ref[head, pl.ds(64, 16), :] = jnp.where(low_rows, d_h, d_l)


def group_reads(pairs, hold, p_ref, o_ref):
    f_ref, g_ref, qs_ref, w_ref, n_ref = hold
    row, col = iotas()
    first = col < 64
    within = row >= col
    for pair in pairs:
        g_h, g_l = g_ref[pair, :, pl.ds(0, C)], g_ref[pair, :, pl.ds(C, C)]
        gg = lanes_of(g_h, g_h)
        f_h, f_l = f_ref[pair, :, pl.ds(0, C)], f_ref[pair, :, pl.ds(C, C)]
        outs = []
        for i in range(2):
            a_h, a_l = masked(f_h, i), masked(f_l, i)
            g = nt(lanes_of(a_h, a_l), gg) + nt(a_h, g_l)
            rk_h, rk_l = split(jnp.where(within, g[:, :C], 0.0))
            re_h, re_l = split(jnp.where(within, g[:, C:], 0.0))
            w_h = w_ref[2 * pair + i]
            outs.append(nn(lanes_of(re_h, rk_h), w_h) + nn(lanes_of(re_l, rk_l), w_h) + nn(re_h, n_ref[2 * pair + i]))
        p_ref[pair] = lanes_of(*split(qs_ref[pair] + jnp.where(first, outs[0], outs[1])))
        o_ref[pair] = roll_half(jnp.where(first, outs[1], outs[0]))


def compose_chunks(odd, msg_ref, zs_ref, g_ref):
    row = lax.broadcasted_iota(jnp.int32, (64, C), 0)
    col = lax.broadcasted_iota(jnp.int32, (64, C), 1)
    left = col < 64
    groups, per = 4, 8
    state = [jnp.where(row == col, 1.0, 0.0) for _ in range(groups)]
    zero = jnp.zeros((64, C), BF16)
    for step in range(per):
        for g in range(groups):
            c = g * per + step
            g_ref[g, pl.ds(64 * step, 64), :] = state[g]
            m = msg_ref[c, pl.ds(0, 64), :].astype(F32)
            tile = msg_ref[c, pl.ds(64, 16), :].astype(F32)
            d = tile[0:1, :] + tile[8:9, :]
            m = jnp.where(odd, roll_half(m), m)
            d = jnp.where(odd, roll_half(jnp.broadcast_to(d, (8, C)))[0:1, :], d)
            trans = jnp.where(left, m + jnp.where(row == col, d, 0.0), 0.0)
            add = jnp.where(left, 0.0, m)
            t_h, t_l = split(trans)
            lhs = lanes_of(jnp.where(left, t_h.astype(F32), roll_half(t_l.astype(F32))).astype(BF16), t_h)
            s_h, s_l = split(state[g])
            state[g] = nn(lhs, rows_of(s_h, s_h, s_l, zero)) + add
    starts = [None]
    z = jnp.where(left, roll_half(state[0]), 0.0)
    for g in range(1, groups):
        starts.append(z)
        if g < groups - 1:
            z = jnp.where(left, apply_state(state[g], z, left) + roll_half(state[g]), 0.0)
    for g in range(groups):
        stack = g_ref[g]
        wide = lax.broadcasted_iota(jnp.int32, (64 * per, C), 1) < 64
        total = roll_half(stack)
        if g > 0:
            total = total + apply_state(stack, starts[g], wide)
        for step in range(per):
            zc = total[64 * step : 64 * step + 64]
            packed = jnp.where(left[:32], zc[:32], roll_half(zc[32:]))
            zs_ref[g * per + step] = packed.astype(BF16)


def apply_state(stack, z, left):
    t_h, t_l = split(jnp.where(left, stack, 0.0))
    z_h, z_l = split(z)
    zero = jnp.zeros((64, C), BF16)
    lhs = lanes_of(jnp.where(left, t_h.astype(F32), roll_half(t_l.astype(F32))).astype(BF16), t_h)
    return nn(lhs, rows_of(z_h, z_h, z_l, zero))


GF = GROUP = 4


def group_finish(pairs, z_ref, p_ref, o_ref, gain_ref, mix_ref):
    row, col = iotas()
    left = lax.broadcasted_iota(jnp.int32, (32, C), 1) < 64
    mean_w = jnp.where((row < 64) == (col < 64), 1.0 / 64, 0.0).astype(BF16)
    mean_w = rows_of(mean_w, mean_w)
    reads = []
    for pair in pairs:
        za = z_ref[2 * pair].astype(F32)
        zb = z_ref[2 * pair + 1].astype(F32)
        zw = rows_of(
            jnp.where(left, za, 0.0),
            jnp.where(left, roll_half(za), 0.0),
            jnp.where(left, 0.0, roll_half(zb)),
            jnp.where(left, 0.0, zb),
        ).astype(BF16)
        reads.append(o_ref[pair] + nn(p_ref[pair], rows_of(zw, zw)))
    centred = [r - nn(lanes_of(*split(r)), mean_w) for r in reads]
    var = [nn(lanes_of(*split(c * c)), mean_w) for c in centred]
    for pair, c, v in zip(pairs, centred, var):
        at = pl.ds(pl.multiple_of(pair * C, C), C)
        mix_ref[:, at] = (c * lax.rsqrt(v + 1.0) * gain_ref[pl.ds(pair, 1), :]).astype(BF16)


def project(slot, mix_ref, w_ref, done_ref):
    acc = jnp.zeros((C, 2 * C), F32)
    for k in range(8):
        at = pl.ds(256 * k, 256)
        acc = acc + nn(mix_ref[:, at], lanes_of(w_ref[0, slot, at, :], w_ref[1, slot, at, :]))
    done_ref[slot] = acc.astype(BF16)


def remote(src, dst, send, recv, **where):
    return pltpu.make_async_remote_copy(
        src_ref=src, dst_ref=dst, send_sem=send, recv_sem=recv, device_id=where, device_id_type=MESH
    )


def kernel(
    q_in,
    k_in,
    v_in,
    dl_in,
    rl_in,
    du_in,
    ru_in,
    base_in,
    gain_in,
    weight_ref,
    out_ref,
    q_ref,
    k_ref,
    v_ref,
    dl_ref,
    rl_ref,
    du_ref,
    ru_ref,
    base_ref,
    gain_ref,
    done_ref,
    in_sem,
    out_sem,
    sq_ref,
    msg_ref,
    got_ref,
    group_ref,
    zs_ref,
    zgot_ref,
    p_ref,
    o_ref,
    mix_ref,
    wall_ref,
    f_ref,
    g_ref,
    qs_ref,
    w_ref,
    n_ref,
    own_sem,
    msg_send,
    msg_recv,
    z_send,
    z_recv,
    ring_send,
    ring_recv,
    quarter_send,
    quarter_recv,
    side_send,
    side_recv,
):
    me = lax.axis_index("sp")
    dp = lax.axis_index("dp")
    core = lax.rem(dp, 2)
    chip = lax.div(dp, 2)
    partner = dp + 1 - 2 * core
    up = lax.rem(dp + 2, DPN)
    down = lax.rem(dp + DPN - 2, DPN)

    inputs = [
        pltpu.make_async_copy(src, dst, in_sem.at[n])
        for n, (src, dst) in enumerate(
            (
                (dl_in, dl_ref),
                (rl_in, rl_ref),
                (du_in, du_ref),
                (ru_in, ru_ref),
                (base_in, base_ref),
                (gain_in, gain_ref),
                (k_in, k_ref),
                (q_in, q_ref),
                (v_in, v_ref),
            )
        )
    ]
    barrier = pltpu.get_barrier_semaphore()

    @pl.loop(1, SP)
    def _(j):
        pl.semaphore_signal(
            barrier, inc=1, device_id={"sp": lax.rem(me + j, SP)}, device_id_type=MESH
        )

    for other in (partner, up, down):
        pl.semaphore_signal(barrier, inc=1, device_id={"dp": other}, device_id_type=MESH)
    own = pltpu.make_async_copy(weight_ref, wall_ref.at[core, 0], own_sem)
    own.start()
    for copy in inputs:
        copy.start()
    inputs[0].wait()
    sq_ref[...] = jnp.tanh(dl_ref[...].astype(F32)).astype(BF16)
    with jax.named_scope("entry"):
        own.wait()
        for copy in inputs[1:]:
            copy.wait()
        pl.semaphore_wait(barrier, SP + 2)

    across = lax.rem(me, 4)
    def rows(slot, start, count):
        return wall_ref.at[core, slot, pl.ds(pl.multiple_of(start, QUARTER // 2), count), :]

    def ring(way, order):
        near = order // 2
        half = order % 2 if way == 0 else 1 - order % 2
        src, dst = ((YN - near) % YN, YN - 1 - near) if way == 0 else (near, near + 1)
        spans = ((WHOLE // 2 * half, WHOLE // 2), (WHOLE + QUARTER * across + QUARTER // 2 * half, QUARTER // 2))
        return [
            remote(
                rows(src, *spans[kind]),
                rows(dst, *spans[kind]),
                ring_send.at[kind, way, order],
                ring_recv.at[kind, way, order],
                dp=(up, down)[way],
            )
            for kind in range(2)
        ]

    def quarter(hop, slot):
        ref = rows(slot, WHOLE + QUARTER * across, QUARTER)
        there = me - across + lax.rem(across + hop + 1, 4)
        return remote(ref, ref, quarter_send.at[hop, slot], quarter_recv.at[hop, slot], sp=there)

    def side(slot, to_me=False):
        start, count = ((0, WHOLE) if slot < YN else (WHOLE, 2048 - WHOLE)) if slot in (4, YN) else (0, 2048)
        ref = wall_ref.at[1 - core if to_me else core, slot % YN if slot < YN else 4, pl.ds(start, count), :]
        return remote(ref, ref, side_send.at[slot], side_recv.at[slot], dp=partner)

    def ring_step(s):
        with jax.named_scope("ring" + str(s)):
            for way in range(2):
                for copy in ring(way, s):
                    copy.wait_recv()
                if s < 5:
                    for copy in ring(way, s + 2):
                        copy.start()

    def share(*slots):
        for slot in slots:
            for hop in range(3):
                quarter(hop, slot).start()

    def complete(*slots):
        with jax.named_scope("complete"):
            for slot in slots:
                for hop in range(3):
                    quarter(hop, slot).wait_recv()
                side(YN if slot == 4 else slot).start()

    for way in range(2):
        for order in range(2):
            for copy in ring(way, order):
                copy.start()
    side(0).start()

    def send_message(head):
        return remote(
            msg_ref.at[head], got_ref.at[me], msg_send.at[head], msg_recv.at[me], sp=head
        )

    def send_pair(pair):
        for i in range(2):
            head = 2 * pair + i

            @pl.when(head != me)
            def _():
                send_message(head).start()

    first_pair = lax.div(me, 2)
    hold = (f_ref, g_ref, qs_ref, w_ref, n_ref)
    refs = (q_ref, k_ref, v_ref, sq_ref, rl_ref, du_ref, ru_ref, base_ref)

    def pairs_of(i):
        return [lax.rem(first_pair + o, PAIRS) for o in (8 - 2 * i, 9 + 2 * i, 7 - 2 * i, 10 + 2 * i)]

    def send_group(i):
        for pair in pairs_of(i):
            send_pair(pair)

    @pl.loop(0, PAIRS // GROUP)
    def _(i):
        @pl.when(i > 0)
        def _():
            send_group(i - 1)

        @pl.when(i == 2)
        def _():
            ring_step(0)

        @pl.when(i == 3)
        def _():
            ring_step(1)
            share(7, 1)

        with jax.named_scope('group'):
            group_states(pairs_of(i), refs, msg_ref, hold)

    got_ref[me] = msg_ref[me]
    send_group(PAIRS // GROUP - 1)
    ring_step(2)

    def reads(i):
        with jax.named_scope("reads"):
            group_reads([GROUP * i + j for j in range(GROUP)], hold, p_ref, o_ref)

    reads(0)
    complete(7, 1)
    reads(1)
    ring_step(3)
    share(6, 2)

    with jax.named_scope('msgwait'):
     @pl.loop(1, SP)
     def _(j):
        other = lax.rem(me + j, SP)
        remote(
            msg_ref.at[me], got_ref.at[other], msg_send.at[other], msg_recv.at[other], sp=other
        ).wait_recv()

    with jax.named_scope('scan'):
        compose_chunks(lax.rem(me, 2) == 1, got_ref, zs_ref, group_ref)

    def send_state(chunk):
        return remote(
            zs_ref.at[chunk], zgot_ref.at[me], z_send.at[chunk], z_recv.at[me], sp=chunk
        )

    zgot_ref[me] = zs_ref[me]

    send_state(lax.rem(me + 16, SP)).start()

    @pl.loop(1, 16)
    def _(j):
        send_state(lax.rem(me + 16 + j, SP)).start()
        send_state(lax.rem(me + 16 - j, SP)).start()

    reads(2)
    ring_step(4)
    complete(6, 2)
    reads(3)

    ring_step(5)
    share(5, 3)

    def wait_state(head):
        @pl.when(head != me)
        def _():
            remote(
                zs_ref.at[me], zgot_ref.at[head], z_send.at[head], z_recv.at[head], sp=head
            ).wait_recv()

    def finish(i):
        with jax.named_scope("zwait"):
            for pair in pairs_of(i):
                wait_state(2 * pair)
                wait_state(2 * pair + 1)
        with jax.named_scope("finish"):
            group_finish(pairs_of(i), zgot_ref, p_ref, o_ref, gain_ref, mix_ref)

    pl.loop(0, 2)(finish)
    ring_step(6)
    share(4)
    side(4).start()
    complete(5, 3)
    pl.loop(2, PAIRS // GROUP)(finish)

    def put_out(slot):
        at = pl.ds(pl.multiple_of(lax.rem(chip + slot, YN) * 256, 256), 256)
        return pltpu.make_async_copy(done_ref.at[slot], out_ref.at[:, at], out_sem.at[slot])

    def project_slots(*slots):
        for slot in slots:
            side(slot, True).wait_recv()
            if slot == 4:
                side(YN, True).wait_recv()
        with jax.named_scope("project"):
            for slot in slots:
                project(slot, mix_ref, wall_ref, done_ref)
                put_out(slot).start()

    project_slots(0, 7, 1)
    complete(4)
    project_slots(6, 2, 5, 3)
    project_slots(4)
    with jax.named_scope("outwait"):
        for slot in range(YN):
            put_out(slot).wait()

    with jax.named_scope("tail"):
        @pl.loop(1, SP)
        def _(j):
            other = lax.rem(me + j, SP)
            send_message(other).wait_send()
            send_state(other).wait_send()

    with jax.named_scope("sent"):
        for way in range(2):
            for order in range(7):
                for copy in ring(way, order):
                    copy.wait_send()
        for slot in range(1, YN):
            for hop in range(3):
                quarter(hop, slot).wait_send()
        for slot in range(YN + 1):
            side(slot).wait_send()


def per_device(query, key, value, decay_low, rate_low, decay_up, rate_up, base, gain, weight):
    dma = pltpu.SemaphoreType.DMA
    out = pl.pallas_call(
        kernel,
        out_shape=jax.ShapeDtypeStruct((C, 2048), BF16),
        in_specs=[pl.BlockSpec(memory_space=pl.ANY)] * 10,
        out_specs=pl.BlockSpec(memory_space=pl.ANY),
        scratch_shapes=[
            pltpu.VMEM((C, 2048), BF16),
            pltpu.VMEM((C, 2048), BF16),
            pltpu.VMEM((C, 2048), BF16),
            pltpu.VMEM((C, C), BF16),
            pltpu.VMEM((C, C), BF16),
            pltpu.VMEM((C, 2048), BF16),
            pltpu.VMEM((C, 2048), BF16),
            pltpu.VMEM((PAIRS, C), F32),
            pltpu.VMEM((PAIRS, C), F32),
            pltpu.VMEM((YN, C, 2 * C), BF16),
            dma((9,)),
            dma((YN,)),
            pltpu.VMEM((C, C), BF16),
            pltpu.VMEM((SP, MSG, C), BF16),
            pltpu.VMEM((SP, MSG, C), BF16),
            pltpu.VMEM((4, 512, C), F32),
            pltpu.VMEM((SP, 32, C), BF16),
            pltpu.VMEM((SP, 32, C), BF16),
            pltpu.VMEM((PAIRS, C, 2 * C), BF16),
            pltpu.VMEM((PAIRS, C, C), F32),
            pltpu.VMEM((C, 2048), BF16),
            pltpu.VMEM((2, YN, 2048, C), BF16),
            pltpu.VMEM((PAIRS, C, 2 * C), BF16),
            pltpu.VMEM((PAIRS, 2 * C, 2 * C), BF16),
            pltpu.VMEM((PAIRS, C, C), F32),
            pltpu.VMEM((SP, 2 * C, C), BF16),
            pltpu.VMEM((SP, C, C), BF16),
            dma,
            dma((SP,)),
            dma((SP,)),
            dma((SP,)),
            dma((SP,)),
            dma((2, 2, 7)),
            dma((2, 2, 7)),
            dma((3, YN)),
            dma((3, YN)),
            dma((YN + 1,)),
            dma((YN + 1,)),
        ],
        compiler_params=pltpu.CompilerParams(
            collective_id=0, has_side_effects=True, vmem_limit_bytes=60 * 2**20
        ),
        name="mixer",
    )(
        query[0],
        key[0],
        value[0],
        decay_low[0],
        rate_low[0],
        decay_up,
        rate_up,
        base.reshape(PAIRS, C),
        gain.reshape(PAIRS, C),
        weight,
    )
    return out[None]


def solution(mesh):
    placed = (P("dp", "sp", None),) * 5 + (P(),) * 4 + (P(None, "dp"),)
    return jax.shard_map(
        per_device, mesh=mesh, in_specs=placed, out_specs=P("dp", "sp", None), check_vma=False
    )
```

```python
import jax
import jax.numpy as jnp
from jax import lax
from jax.experimental import pallas as pl
from jax.experimental.pallas import tpu as pltpu
from jax.sharding import PartitionSpec as P

F32 = jnp.float32
BF16 = jnp.bfloat16
C = 128
PAIRS = 16
SP = 32
DPN = 16
YN = 8
MSG = 80
WHOLE = 512
PART = (2048 - WHOLE) // 4
DECAY_SCALE = 0.6065306597126334
MESH = pl.DeviceIdType.MESH


def split(x):
    high = x.astype(BF16)
    return high, (x - high.astype(F32)).astype(BF16)


def nn(a, b):
    return jnp.dot(a, b, preferred_element_type=F32)


def nt(a, b):
    return lax.dot_general(a, b, (((1,), (1,)), ((), ())), preferred_element_type=F32)


def rows_of(*parts):
    return jnp.concatenate(parts, axis=0)


def lanes_of(*parts):
    return jnp.concatenate(parts, axis=1)


def sigmoid(x):
    return 1.0 / (1.0 + jnp.exp(-x))


def iotas():
    return (
        lax.broadcasted_iota(jnp.int32, (C, C), 0),
        lax.broadcasted_iota(jnp.int32, (C, C), 1),
    )


def roll_half(x):
    return pltpu.roll(x, 64, 1)


def pair_front(pair, q_ref, k_ref, v_ref, sq_ref, rl_ref, du_ref, ru_ref, base_ref):
    row, col = iotas()
    first = col < 64
    at = pl.ds(pl.multiple_of(pair * C, C), C)
    decay_pre = (base_ref[pl.ds(pair, 1), :] + nn(sq_ref[...], du_ref[:, at])).astype(BF16).astype(F32)
    rate_pre = nn(rl_ref[...], ru_ref[:, at]).astype(BF16).astype(F32)
    log_decay = -DECAY_SCALE * sigmoid(decay_pre)
    rate = sigmoid(rate_pre)
    tri = jnp.where(row >= col, 1.0, 0.0).astype(BF16)
    ld_h, ld_l = split(log_decay)
    running = nn(lanes_of(tri, tri), rows_of(ld_h, ld_l))
    key = k_ref[:, at].astype(F32)
    query = q_ref[:, at].astype(F32)
    same = jnp.where((row < 64) == first, 1.0, 0.0).astype(BF16)
    sq_h, sq_l = split(key * key)
    unit = key * lax.rsqrt(1.0 + nn(lanes_of(sq_h, sq_l), rows_of(same, same)))
    erase = unit * rate
    centre = running[63:64, :]
    final = running[C - 1 : C, :]
    up = jnp.exp(running - centre)
    down = jnp.exp(centre - running)
    before = jnp.exp(running - log_decay - centre)
    from_start = jnp.exp(centre)
    to_end = jnp.exp(final - centre)
    f1 = unit * before
    f2 = query * up
    g1 = key * down
    g2 = erase * down
    return f1, f2, g1, g2, f1 * from_start, f2 * from_start, g1 * to_end, g2 * to_end, jnp.exp(final)


def invert_unit_lower(lows):
    row, col = iotas()
    differ = row ^ col
    zero = jnp.zeros((C, C), BF16)
    lane16 = lax.broadcasted_iota(jnp.int32, (16, C), 1)
    row16 = lax.broadcasted_iota(jnp.int32, (16, C), 0)
    inner = row16 ^ (lane16 & 15)

    def gather(low):
        out = low[0:16]
        for b in range(1, 8):
            out = jnp.where((lane16 >> 4) == b, low[16 * b : 16 * b + 16], out)
        return out

    def spread(small, size):
        own = (row // size) == (col // size)
        tiled = rows_of(*[small.astype(BF16)] * (C // size)) if size < C else small.astype(BF16)
        return jnp.where(own, tiled, zero)

    eye = jnp.where(inner == 0, 1.0, 0.0)
    wide_row = lax.broadcasted_iota(jnp.int32, (C, 16 * C), 0)
    wide_col = lax.broadcasted_iota(jnp.int32, (C, 16 * C), 1)
    pick = (wide_row & 15) == (wide_col // C)
    pick = jnp.where(pick & ((wide_row >> 4) == ((wide_col % C) >> 4)), 1.0, 0.0).astype(BF16)
    packed = [gather(low) for low in lows]
    columns = nn(rows_of(*packed), pick)
    small = []
    for n in range(len(lows)):
        x = eye
        for s in range(15):
            x = x - columns[16 * n : 16 * n + 16, C * s : C * s + C] * x[s : s + 1]
        small.append(x)
    size = 16
    while size < C:
        level = (differ >= size) & (differ < 2 * size)
        even = (lax.broadcasted_iota(jnp.int32, (size, C), 1) & size) == 0
        mid = [
            nn(jnp.where(even, 0.0, s).astype(BF16), jnp.where(level, low, zero)).astype(BF16)
            for s, low in zip(small, lows)
        ]
        corner = [nn(m, spread(s, size)) for s, m in zip(small, mid)]
        small = [rows_of(jnp.where(even, s, 0.0), jnp.where(even, -c, s)) for s, c in zip(small, corner)]
        size *= 2
    return [s.astype(BF16) for s in small]


def masked(x, i):
    first = lax.broadcasted_iota(jnp.int32, x.shape, 1) < 64
    zero = jnp.zeros(x.shape, x.dtype)
    return jnp.where(first, x, zero) if i == 0 else jnp.where(first, zero, x)


def grams_of(f_h, f_l, gg, g_l):
    high = rows_of(masked(f_h, 0), masked(f_h, 1))
    low = rows_of(masked(f_l, 0), masked(f_l, 1))
    g = nt(lanes_of(high, low), gg) + nt(high, g_l)
    return g[:C], g[C:]


def group_states(pairs, refs, msg_ref, hold):
    f_ref, g_ref, qs_ref, w_ref, n_ref = hold
    v_ref = refs[2]
    row, col = iotas()
    first = col < 64
    strict = row > col
    ep, kp, ends, v_rolls = [], [], [], []
    for pair in pairs:
        at = pl.ds(pl.multiple_of(pair * C, C), C)
        f1, f2, g1, g2, es, qs, ke, ee, efin = pair_front(pair, *refs)
        qs_ref[pair] = qs
        f_ref[pair] = lanes_of(*split(f2))
        ends.append((es, ke, ee, efin))
        v_rolls.append(roll_half(v_ref[:, at].astype(F32)).astype(BF16))
        f_h, f_l = split(f1)
        g_h, g_l = split(rows_of(g1, g2))
        g_ref[pair] = lanes_of(g_h, g_l)
        gg = lanes_of(g_h, g_h)
        for g in grams_of(f_h, f_l, gg, g_l):
            kp.append(split(jnp.where(strict, g[:, :C], 0.0)))
            ep.append(split(jnp.where(strict, g[:, C:], 0.0)))
    heads = range(2 * len(pairs))
    carried = [nn(lanes_of(*kp[n]), rows_of(v_rolls[n // 2], v_rolls[n // 2])) for n in heads]
    xb = invert_unit_lower([e[0] for e in ep])
    rhs = [
        jnp.where(first, ends[n // 2][0], carried[n]) if n % 2 == 0 else jnp.where(first, carried[n], ends[n // 2][0])
        for n in heads
    ]
    s0 = [nn(xb[n], rhs[n].astype(BF16)).astype(BF16) for n in heads]
    resid = [rhs[n] - s0[n].astype(F32) - nn(lanes_of(*ep[n]), rows_of(s0[n], s0[n])) for n in heads]
    sol = [s0[n].astype(F32) + nn(xb[n], resid[n].astype(BF16)) for n in heads]
    low_rows = lax.broadcasted_iota(jnp.int32, (16, C), 0) < 8
    for n in heads:
        _, ke, ee, efin = ends[n // 2]
        head = 2 * pairs[n // 2] + n % 2
        half = slice(64 * (n % 2), 64 * (n % 2) + 64)
        ee_h, ee_l = split(ee.T[half])
        ke_h, ke_l = split(ke.T[half])
        n_h, n_l = split(-sol[n])
        w_h = rows_of(n_h, masked(v_rolls[n // 2], 1 - n % 2))
        w_ref[head] = w_h
        n_ref[head] = n_l
        out = nn(lanes_of(ee_h, ke_h), w_h) + nn(lanes_of(ee_l, ke_l), w_h) + nn(ee_h, n_l)
        d_h, d_l = split(jnp.broadcast_to(efin, (16, C)))
        msg_ref[head, pl.ds(0, 64), :] = out.astype(BF16)
        msg_ref[head, pl.ds(64, 16), :] = jnp.where(low_rows, d_h, d_l)


def group_reads(pairs, hold, p_ref, o_ref):
    f_ref, g_ref, qs_ref, w_ref, n_ref = hold
    row, col = iotas()
    first = col < 64
    within = row >= col
    for pair in pairs:
        g_h, g_l = g_ref[pair, :, pl.ds(0, C)], g_ref[pair, :, pl.ds(C, C)]
        gg = lanes_of(g_h, g_h)
        f_h, f_l = f_ref[pair, :, pl.ds(0, C)], f_ref[pair, :, pl.ds(C, C)]
        outs = []
        for i, g in enumerate(grams_of(f_h, f_l, gg, g_l)):
            rk_h, rk_l = split(jnp.where(within, g[:, :C], 0.0))
            re_h, re_l = split(jnp.where(within, g[:, C:], 0.0))
            w_h = w_ref[2 * pair + i]
            outs.append(nn(lanes_of(re_h, rk_h), w_h) + nn(lanes_of(re_l, rk_l), w_h) + nn(re_h, n_ref[2 * pair + i]))
        p_ref[pair] = lanes_of(*split(qs_ref[pair] + jnp.where(first, outs[0], outs[1])))
        o_ref[pair] = roll_half(jnp.where(first, outs[1], outs[0]))


def compose_chunks(odd, msg_ref, zs_ref, g_ref):
    row = lax.broadcasted_iota(jnp.int32, (64, C), 0)
    col = lax.broadcasted_iota(jnp.int32, (64, C), 1)
    left = col < 64
    groups, per = 4, 8
    state = [jnp.where(row == col, 1.0, 0.0) for _ in range(groups)]
    zero = jnp.zeros((64, C), BF16)
    for step in range(per):
        for g in range(groups):
            c = g * per + step
            g_ref[g, pl.ds(64 * step, 64), :] = state[g]
            m = msg_ref[c, pl.ds(0, 64), :].astype(F32)
            tile = msg_ref[c, pl.ds(64, 16), :].astype(F32)
            d = tile[0:1, :] + tile[8:9, :]
            m = jnp.where(odd, roll_half(m), m)
            d = jnp.where(odd, roll_half(jnp.broadcast_to(d, (8, C)))[0:1, :], d)
            trans = jnp.where(left, m + jnp.where(row == col, d, 0.0), 0.0)
            add = jnp.where(left, 0.0, m)
            t_h, t_l = split(trans)
            lhs = lanes_of(jnp.where(left, t_h.astype(F32), roll_half(t_l.astype(F32))).astype(BF16), t_h)
            s_h, s_l = split(state[g])
            state[g] = nn(lhs, rows_of(s_h, s_h, s_l, zero)) + add
    starts = [None]
    z = jnp.where(left, roll_half(state[0]), 0.0)
    for g in range(1, groups):
        starts.append(z)
        if g < groups - 1:
            z = jnp.where(left, apply_state(state[g], z, left) + roll_half(state[g]), 0.0)
    for g in range(groups):
        stack = g_ref[g]
        wide = lax.broadcasted_iota(jnp.int32, (64 * per, C), 1) < 64
        total = roll_half(stack)
        if g > 0:
            total = total + apply_state(stack, starts[g], wide)
        for step in range(per):
            zc = total[64 * step : 64 * step + 64]
            packed = jnp.where(left[:32], zc[:32], roll_half(zc[32:]))
            zs_ref[g * per + step] = packed.astype(BF16)


def apply_state(stack, z, left):
    t_h, t_l = split(jnp.where(left, stack, 0.0))
    z_h, z_l = split(z)
    zero = jnp.zeros((64, C), BF16)
    lhs = lanes_of(jnp.where(left, t_h.astype(F32), roll_half(t_l.astype(F32))).astype(BF16), t_h)
    return nn(lhs, rows_of(z_h, z_h, z_l, zero))


GF = GROUP = 4


def group_finish(pairs, z_ref, p_ref, o_ref, gain_ref, mix_ref):
    row, col = iotas()
    left = lax.broadcasted_iota(jnp.int32, (32, C), 1) < 64
    mean_w = jnp.where((row < 64) == (col < 64), 1.0 / 64, 0.0).astype(BF16)
    mean_w = rows_of(mean_w, mean_w)
    reads = []
    for pair in pairs:
        za = z_ref[2 * pair].astype(F32)
        zb = z_ref[2 * pair + 1].astype(F32)
        zw = rows_of(
            jnp.where(left, za, 0.0),
            jnp.where(left, roll_half(za), 0.0),
            jnp.where(left, 0.0, roll_half(zb)),
            jnp.where(left, 0.0, zb),
        ).astype(BF16)
        reads.append(o_ref[pair] + nn(p_ref[pair], rows_of(zw, zw)))
    centred = [r - nn(lanes_of(*split(r)), mean_w) for r in reads]
    var = [nn(lanes_of(*split(c * c)), mean_w) for c in centred]
    for pair, c, v in zip(pairs, centred, var):
        at = pl.ds(pl.multiple_of(pair * C, C), C)
        mix_ref[:, at] = (c * lax.rsqrt(v + 1.0) * gain_ref[pl.ds(pair, 1), :]).astype(BF16)


def project(slot, mix_ref, w_ref, done_ref):
    acc = jnp.zeros((C, 2 * C), F32)
    for k in range(8):
        at = pl.ds(256 * k, 256)
        acc = acc + nn(mix_ref[:, at], lanes_of(w_ref[0, slot, at, :], w_ref[1, slot, at, :]))
    done_ref[slot] = acc.astype(BF16)


def remote(src, dst, send, recv, **where):
    return pltpu.make_async_remote_copy(
        src_ref=src, dst_ref=dst, send_sem=send, recv_sem=recv, device_id=where, device_id_type=MESH
    )


def kernel(
    q_in,
    k_in,
    v_in,
    dl_in,
    rl_in,
    du_in,
    ru_in,
    base_in,
    gain_in,
    weight_ref,
    out_ref,
    q_ref,
    k_ref,
    v_ref,
    dl_ref,
    rl_ref,
    du_ref,
    ru_ref,
    base_ref,
    gain_ref,
    done_ref,
    in_sem,
    out_sem,
    sq_ref,
    msg_ref,
    got_ref,
    group_ref,
    zs_ref,
    zgot_ref,
    p_ref,
    o_ref,
    mix_ref,
    wall_ref,
    f_ref,
    g_ref,
    qs_ref,
    w_ref,
    n_ref,
    own_sem,
    msg_send,
    msg_recv,
    z_send,
    z_recv,
    ring_send,
    ring_recv,
    swap_send,
    swap_recv,
    side_send,
    side_recv,
):
    me = lax.axis_index("sp")
    dp = lax.axis_index("dp")
    core = lax.rem(dp, 2)
    chip = lax.div(dp, 2)
    partner = dp + 1 - 2 * core
    up = lax.rem(dp + 2, DPN)
    down = lax.rem(dp + DPN - 2, DPN)

    inputs = [
        pltpu.make_async_copy(src, dst, in_sem.at[n])
        for n, (src, dst) in enumerate(
            (
                (dl_in, dl_ref),
                (rl_in, rl_ref),
                (du_in, du_ref),
                (ru_in, ru_ref),
                (base_in, base_ref),
                (gain_in, gain_ref),
                (k_in, k_ref),
                (q_in, q_ref),
                (v_in, v_ref),
            )
        )
    ]
    barrier = pltpu.get_barrier_semaphore()

    @pl.loop(1, SP)
    def _(j):
        pl.semaphore_signal(
            barrier, inc=1, device_id={"sp": lax.rem(me + j, SP)}, device_id_type=MESH
        )

    for other in (partner, up, down):
        pl.semaphore_signal(barrier, inc=1, device_id={"dp": other}, device_id_type=MESH)
    own = pltpu.make_async_copy(weight_ref, wall_ref.at[core, 0], own_sem)
    own.start()
    for copy in inputs:
        copy.start()
    inputs[0].wait()
    sq_ref[...] = jnp.tanh(dl_ref[...].astype(F32)).astype(BF16)
    with jax.named_scope("entry"):
        own.wait()
        for copy in inputs[1:]:
            copy.wait()
        pl.semaphore_wait(barrier, SP + 2)

    across = lax.rem(me, 4)
    parity = lax.rem(across, 2)

    def rows(slot, start, count):
        return wall_ref.at[core, slot, pl.ds(pl.multiple_of(start, 16), count), :]

    def ring(way, order):
        near = order // 2
        half = order % 2 if way == 0 else 1 - order % 2
        src, dst = ((YN - near) % YN, YN - 1 - near) if way == 0 else (near, near + 1)
        spans = ((WHOLE // 2 * half, WHOLE // 2), (WHOLE + 2 * PART * parity + PART * half, PART))
        return [
            remote(
                rows(src, *spans[kind]),
                rows(dst, *spans[kind]),
                ring_send.at[kind, way, order],
                ring_recv.at[kind, way, order],
                dp=(up, down)[way],
            )
            for kind in range(2)
        ]

    def swap(hop, slot):
        ref = rows(slot, WHOLE + 2 * PART * parity + PART * hop, PART)
        there = me - across + lax.rem(across + 1 + 2 * hop, 4)
        return remote(ref, ref, swap_send.at[hop, slot], swap_recv.at[hop, slot], sp=there)

    def side(slot, to_me=False):
        start, count = ((0, WHOLE) if slot < YN else (WHOLE, 2048 - WHOLE)) if slot in (4, YN) else (0, 2048)
        ref = wall_ref.at[1 - core if to_me else core, slot % YN if slot < YN else 4, pl.ds(start, count), :]
        return remote(ref, ref, side_send.at[slot], side_recv.at[slot], dp=partner)

    def ring_step(s):
        with jax.named_scope("ring" + str(s)):
            for way in range(2):
                for copy in ring(way, s):
                    copy.wait_recv()
                if s < 5:
                    for copy in ring(way, s + 2):
                        copy.start()

    def share(*slots):
        for slot in slots:
            for hop in range(2):
                swap(hop, slot).start()

    def complete(*slots):
        with jax.named_scope("complete"):
            for slot in slots:
                for hop in range(2):
                    swap(hop, slot).wait_recv()
                side(YN if slot == 4 else slot).start()

    for way in range(2):
        for order in range(2):
            for copy in ring(way, order):
                copy.start()
    side(0).start()

    def send_message(head):
        return remote(
            msg_ref.at[head], got_ref.at[me], msg_send.at[head], msg_recv.at[me], sp=head
        )

    def send_pair(pair):
        for i in range(2):
            head = 2 * pair + i

            @pl.when(head != me)
            def _():
                send_message(head).start()

    first_pair = lax.div(me, 2)
    hold = (f_ref, g_ref, qs_ref, w_ref, n_ref)
    refs = (q_ref, k_ref, v_ref, sq_ref, rl_ref, du_ref, ru_ref, base_ref)

    def pairs_of(i):
        return [lax.rem(first_pair + o, PAIRS) for o in (8 - 2 * i, 9 + 2 * i, 7 - 2 * i, 10 + 2 * i)]

    def send_group(i):
        for pair in pairs_of(i):
            send_pair(pair)

    @pl.loop(0, PAIRS // GROUP)
    def _(i):
        @pl.when(i > 0)
        def _():
            send_group(i - 1)

        @pl.when(i == 2)
        def _():
            ring_step(0)

        @pl.when(i == 3)
        def _():
            ring_step(1)
            share(7, 1)

        with jax.named_scope('group'):
            group_states(pairs_of(i), refs, msg_ref, hold)

    got_ref[me] = msg_ref[me]
    send_group(PAIRS // GROUP - 1)
    ring_step(2)

    def reads(i):
        with jax.named_scope("reads"):
            group_reads([GROUP * i + j for j in range(GROUP)], hold, p_ref, o_ref)

    reads(0)
    reads(1)
    ring_step(3)
    share(6, 2)

    with jax.named_scope('msgwait'):
     @pl.loop(1, SP)
     def _(j):
        other = lax.rem(me + j, SP)
        remote(
            msg_ref.at[me], got_ref.at[other], msg_send.at[other], msg_recv.at[other], sp=other
        ).wait_recv()

    with jax.named_scope('scan'):
        compose_chunks(lax.rem(me, 2) == 1, got_ref, zs_ref, group_ref)

    def send_state(chunk):
        return remote(
            zs_ref.at[chunk], zgot_ref.at[me], z_send.at[chunk], z_recv.at[me], sp=chunk
        )

    zgot_ref[me] = zs_ref[me]

    send_state(lax.rem(me + 16, SP)).start()

    @pl.loop(1, 16)
    def _(j):
        send_state(lax.rem(me + 16 + j, SP)).start()
        send_state(lax.rem(me + 16 - j, SP)).start()

    ring_step(4)
    reads(2)
    reads(3)
    complete(7, 1)

    ring_step(5)
    share(5, 3)

    def wait_state(head):
        @pl.when(head != me)
        def _():
            remote(
                zs_ref.at[me], zgot_ref.at[head], z_send.at[head], z_recv.at[head], sp=head
            ).wait_recv()

    def finish(i):
        with jax.named_scope("zwait"):
            for pair in pairs_of(i):
                wait_state(2 * pair)
                wait_state(2 * pair + 1)
        with jax.named_scope("finish"):
            group_finish(pairs_of(i), zgot_ref, p_ref, o_ref, gain_ref, mix_ref)

    pl.loop(0, 2)(finish)
    ring_step(6)
    share(4)
    side(4).start()
    complete(6, 2)
    pl.loop(2, PAIRS // GROUP)(finish)
    complete(5, 3)

    def put_out(slot):
        at = pl.ds(pl.multiple_of(lax.rem(chip + slot, YN) * 256, 256), 256)
        return pltpu.make_async_copy(done_ref.at[slot], out_ref.at[:, at], out_sem.at[slot])

    def project_slots(*slots):
        for slot in slots:
            side(slot, True).wait_recv()
            if slot == 4:
                side(YN, True).wait_recv()
        with jax.named_scope("project"):
            for slot in slots:
                project(slot, mix_ref, wall_ref, done_ref)
                put_out(slot).start()

    project_slots(0, 7, 1)
    complete(4)
    project_slots(6, 2, 5, 3)
    project_slots(4)
    with jax.named_scope("outwait"):
        for slot in range(YN):
            put_out(slot).wait()

    with jax.named_scope("tail"):
        @pl.loop(1, SP)
        def _(j):
            other = lax.rem(me + j, SP)
            send_message(other).wait_send()
            send_state(other).wait_send()

    with jax.named_scope("sent"):
        for way in range(2):
            for order in range(7):
                for copy in ring(way, order):
                    copy.wait_send()
        for slot in range(1, YN):
            for hop in range(2):
                swap(hop, slot).wait_send()
        for slot in range(YN + 1):
            side(slot).wait_send()


def per_device(query, key, value, decay_low, rate_low, decay_up, rate_up, base, gain, weight):
    dma = pltpu.SemaphoreType.DMA
    out = pl.pallas_call(
        kernel,
        out_shape=jax.ShapeDtypeStruct((C, 2048), BF16),
        in_specs=[pl.BlockSpec(memory_space=pl.ANY)] * 10,
        out_specs=pl.BlockSpec(memory_space=pl.ANY),
        scratch_shapes=[
            pltpu.VMEM((C, 2048), BF16),
            pltpu.VMEM((C, 2048), BF16),
            pltpu.VMEM((C, 2048), BF16),
            pltpu.VMEM((C, C), BF16),
            pltpu.VMEM((C, C), BF16),
            pltpu.VMEM((C, 2048), BF16),
            pltpu.VMEM((C, 2048), BF16),
            pltpu.VMEM((PAIRS, C), F32),
            pltpu.VMEM((PAIRS, C), F32),
            pltpu.VMEM((YN, C, 2 * C), BF16),
            dma((9,)),
            dma((YN,)),
            pltpu.VMEM((C, C), BF16),
            pltpu.VMEM((SP, MSG, C), BF16),
            pltpu.VMEM((SP, MSG, C), BF16),
            pltpu.VMEM((4, 512, C), F32),
            pltpu.VMEM((SP, 32, C), BF16),
            pltpu.VMEM((SP, 32, C), BF16),
            pltpu.VMEM((PAIRS, C, 2 * C), BF16),
            pltpu.VMEM((PAIRS, C, C), F32),
            pltpu.VMEM((C, 2048), BF16),
            pltpu.VMEM((2, YN, 2048, C), BF16),
            pltpu.VMEM((PAIRS, C, 2 * C), BF16),
            pltpu.VMEM((PAIRS, 2 * C, 2 * C), BF16),
            pltpu.VMEM((PAIRS, C, C), F32),
            pltpu.VMEM((SP, 2 * C, C), BF16),
            pltpu.VMEM((SP, C, C), BF16),
            dma,
            dma((SP,)),
            dma((SP,)),
            dma((SP,)),
            dma((SP,)),
            dma((2, 2, 7)),
            dma((2, 2, 7)),
            dma((2, YN)),
            dma((2, YN)),
            dma((YN + 1,)),
            dma((YN + 1,)),
        ],
        compiler_params=pltpu.CompilerParams(
            collective_id=0, has_side_effects=True, vmem_limit_bytes=60 * 2**20
        ),
        name="mixer",
    )(
        query[0],
        key[0],
        value[0],
        decay_low[0],
        rate_low[0],
        decay_up,
        rate_up,
        base.reshape(PAIRS, C),
        gain.reshape(PAIRS, C),
        weight,
    )
    return out[None]


def solution(mesh):
    placed = (P("dp", "sp", None),) * 5 + (P(),) * 4 + (P(None, "dp"),)
    return jax.shard_map(
        per_device, mesh=mesh, in_specs=placed, out_specs=P("dp", "sp", None), check_vma=False
    )
```

```python
import jax
import jax.numpy as jnp
from jax import lax
from jax.experimental import pallas as pl
from jax.experimental.pallas import tpu as pltpu
from jax.sharding import PartitionSpec as P

F32 = jnp.float32
BF16 = jnp.bfloat16
C = 128
PAIRS = 16
SP = 32
DPN = 16
YN = 8
MSG = 80
WHOLE = 512
PART = (2048 - WHOLE) // 4
DECAY_SCALE = 0.6065306597126334
MESH = pl.DeviceIdType.MESH


def split(x):
    high = x.astype(BF16)
    return high, (x - high.astype(F32)).astype(BF16)


def nn(a, b):
    return jnp.dot(a, b, preferred_element_type=F32)


def nt(a, b):
    return lax.dot_general(a, b, (((1,), (1,)), ((), ())), preferred_element_type=F32)


def rows_of(*parts):
    return jnp.concatenate(parts, axis=0)


def lanes_of(*parts):
    return jnp.concatenate(parts, axis=1)


def sigmoid(x):
    return 1.0 / (1.0 + jnp.exp(-x))


def iotas():
    return (
        lax.broadcasted_iota(jnp.int32, (C, C), 0),
        lax.broadcasted_iota(jnp.int32, (C, C), 1),
    )


def roll_half(x):
    return pltpu.roll(x, 64, 1)


def pair_front(pair, q_ref, k_ref, v_ref, sq_ref, rl_ref, du_ref, ru_ref, base_ref):
    row, col = iotas()
    first = col < 64
    at = pl.ds(pl.multiple_of(pair * C, C), C)
    decay_pre = (base_ref[pl.ds(pair, 1), :] + nn(sq_ref[...], du_ref[:, at])).astype(BF16).astype(F32)
    rate_pre = nn(rl_ref[...], ru_ref[:, at]).astype(BF16).astype(F32)
    log_decay = -DECAY_SCALE * sigmoid(decay_pre)
    rate = sigmoid(rate_pre)
    tri = jnp.where(row >= col, 1.0, 0.0).astype(BF16)
    ld_h, ld_l = split(log_decay)
    running = nn(lanes_of(tri, tri), rows_of(ld_h, ld_l))
    key = k_ref[:, at].astype(F32)
    query = q_ref[:, at].astype(F32)
    same = jnp.where((row < 64) == first, 1.0, 0.0).astype(BF16)
    sq_h, sq_l = split(key * key)
    unit = key * lax.rsqrt(1.0 + nn(lanes_of(sq_h, sq_l), rows_of(same, same)))
    erase = unit * rate
    centre = running[63:64, :]
    final = running[C - 1 : C, :]
    up = jnp.exp(running - centre)
    down = jnp.exp(centre - running)
    before = jnp.exp(running - log_decay - centre)
    from_start = jnp.exp(centre)
    to_end = jnp.exp(final - centre)
    f1 = unit * before
    f2 = query * up
    g1 = key * down
    g2 = erase * down
    return f1, f2, g1, g2, f1 * from_start, f2 * from_start, g1 * to_end, g2 * to_end, jnp.exp(final)


def invert_unit_lower(lows):
    row, col = iotas()
    differ = row ^ col
    zero = jnp.zeros((C, C), BF16)
    lane16 = lax.broadcasted_iota(jnp.int32, (16, C), 1)
    row16 = lax.broadcasted_iota(jnp.int32, (16, C), 0)
    inner = row16 ^ (lane16 & 15)

    def gather(low):
        out = low[0:16]
        for b in range(1, 8):
            out = jnp.where((lane16 >> 4) == b, low[16 * b : 16 * b + 16], out)
        return out

    def spread(small, size):
        own = (row // size) == (col // size)
        tiled = rows_of(*[small.astype(BF16)] * (C // size)) if size < C else small.astype(BF16)
        return jnp.where(own, tiled, zero)

    eye = jnp.where(inner == 0, 1.0, 0.0)
    wide_row = lax.broadcasted_iota(jnp.int32, (C, 16 * C), 0)
    wide_col = lax.broadcasted_iota(jnp.int32, (C, 16 * C), 1)
    pick = (wide_row & 15) == (wide_col // C)
    pick = jnp.where(pick & ((wide_row >> 4) == ((wide_col % C) >> 4)), 1.0, 0.0).astype(BF16)
    packed = [gather(low) for low in lows]
    columns = nn(rows_of(*packed), pick)
    small = []
    for n in range(len(lows)):
        x = eye
        for s in range(15):
            x = x - columns[16 * n : 16 * n + 16, C * s : C * s + C] * x[s : s + 1]
        small.append(x)
    size = 16
    while size < C:
        level = (differ >= size) & (differ < 2 * size)
        even = (lax.broadcasted_iota(jnp.int32, (size, C), 1) & size) == 0
        mid = [
            nn(jnp.where(even, 0.0, s).astype(BF16), jnp.where(level, low, zero)).astype(BF16)
            for s, low in zip(small, lows)
        ]
        corner = [nn(m, spread(s, size)) for s, m in zip(small, mid)]
        small = [rows_of(jnp.where(even, s, 0.0), jnp.where(even, -c, s)) for s, c in zip(small, corner)]
        size *= 2
    return [s.astype(BF16) for s in small]


def masked(x, i):
    first = lax.broadcasted_iota(jnp.int32, x.shape, 1) < 64
    zero = jnp.zeros(x.shape, x.dtype)
    return jnp.where(first, x, zero) if i == 0 else jnp.where(first, zero, x)


def grams_of(f_h, f_l, gg, g_l):
    high = rows_of(masked(f_h, 0), masked(f_h, 1))
    low = rows_of(masked(f_l, 0), masked(f_l, 1))
    g = nt(lanes_of(high, low), gg) + nt(high, g_l)
    return g[:C], g[C:]


def group_states(pairs, refs, msg_ref, hold):
    f_ref, g_ref, qs_ref, w_ref, n_ref = hold
    v_ref = refs[2]
    row, col = iotas()
    first = col < 64
    strict = row > col
    ep, kp, ends, v_rolls = [], [], [], []
    for pair in pairs:
        at = pl.ds(pl.multiple_of(pair * C, C), C)
        f1, f2, g1, g2, es, qs, ke, ee, efin = pair_front(pair, *refs)
        qs_ref[pair] = qs
        f_ref[pair] = lanes_of(*split(f2))
        ends.append((es, ke, ee, efin))
        v_rolls.append(roll_half(v_ref[:, at].astype(F32)).astype(BF16))
        f_h, f_l = split(f1)
        g_h, g_l = split(rows_of(g1, g2))
        g_ref[pair] = lanes_of(g_h, g_l)
        gg = lanes_of(g_h, g_h)
        for g in grams_of(f_h, f_l, gg, g_l):
            kp.append(split(jnp.where(strict, g[:, :C], 0.0)))
            ep.append(split(jnp.where(strict, g[:, C:], 0.0)))
    heads = range(2 * len(pairs))
    carried = [nn(lanes_of(*kp[n]), rows_of(v_rolls[n // 2], v_rolls[n // 2])) for n in heads]
    xb = invert_unit_lower([e[0] for e in ep])
    rhs = [
        jnp.where(first, ends[n // 2][0], carried[n]) if n % 2 == 0 else jnp.where(first, carried[n], ends[n // 2][0])
        for n in heads
    ]
    s0 = [nn(xb[n], rhs[n].astype(BF16)).astype(BF16) for n in heads]
    resid = [rhs[n] - s0[n].astype(F32) - nn(lanes_of(*ep[n]), rows_of(s0[n], s0[n])) for n in heads]
    sol = [s0[n].astype(F32) + nn(xb[n], resid[n].astype(BF16)) for n in heads]
    low_rows = lax.broadcasted_iota(jnp.int32, (16, C), 0) < 8
    for n in heads:
        _, ke, ee, efin = ends[n // 2]
        head = 2 * pairs[n // 2] + n % 2
        half = slice(64 * (n % 2), 64 * (n % 2) + 64)
        ee_h, ee_l = split(ee.T[half])
        ke_h, ke_l = split(ke.T[half])
        n_h, n_l = split(-sol[n])
        w_h = rows_of(n_h, masked(v_rolls[n // 2], 1 - n % 2))
        w_ref[head] = w_h
        n_ref[head] = n_l
        out = nn(lanes_of(ee_h, ke_h), w_h) + nn(lanes_of(ee_l, ke_l), w_h) + nn(ee_h, n_l)
        d_h, d_l = split(jnp.broadcast_to(efin, (16, C)))
        msg_ref[head, pl.ds(0, 64), :] = out.astype(BF16)
        msg_ref[head, pl.ds(64, 16), :] = jnp.where(low_rows, d_h, d_l)


def group_reads(pairs, hold, p_ref, o_ref):
    f_ref, g_ref, qs_ref, w_ref, n_ref = hold
    row, col = iotas()
    first = col < 64
    within = row >= col
    for pair in pairs:
        g_h, g_l = g_ref[pair, :, pl.ds(0, C)], g_ref[pair, :, pl.ds(C, C)]
        gg = lanes_of(g_h, g_h)
        f_h, f_l = f_ref[pair, :, pl.ds(0, C)], f_ref[pair, :, pl.ds(C, C)]
        outs = []
        for i, g in enumerate(grams_of(f_h, f_l, gg, g_l)):
            rk_h, rk_l = split(jnp.where(within, g[:, :C], 0.0))
            re_h, re_l = split(jnp.where(within, g[:, C:], 0.0))
            w_h = w_ref[2 * pair + i]
            outs.append(nn(lanes_of(re_h, rk_h), w_h) + nn(lanes_of(re_l, rk_l), w_h) + nn(re_h, n_ref[2 * pair + i]))
        p_ref[pair] = lanes_of(*split(qs_ref[pair] + jnp.where(first, outs[0], outs[1])))
        o_ref[pair] = roll_half(jnp.where(first, outs[1], outs[0]))


def compose_chunks(odd, msg_ref, zs_ref, g_ref):
    row = lax.broadcasted_iota(jnp.int32, (64, C), 0)
    col = lax.broadcasted_iota(jnp.int32, (64, C), 1)
    left = col < 64
    groups, per = 4, 8
    state = [jnp.where(row == col, 1.0, 0.0) for _ in range(groups)]
    zero = jnp.zeros((64, C), BF16)
    for step in range(per):
        for g in range(groups):
            c = g * per + step
            g_ref[g, pl.ds(64 * step, 64), :] = state[g]
            m = msg_ref[c, pl.ds(0, 64), :].astype(F32)
            tile = msg_ref[c, pl.ds(64, 16), :].astype(F32)
            d = tile[0:1, :] + tile[8:9, :]
            m = jnp.where(odd, roll_half(m), m)
            d = jnp.where(odd, roll_half(jnp.broadcast_to(d, (8, C)))[0:1, :], d)
            trans = jnp.where(left, m + jnp.where(row == col, d, 0.0), 0.0)
            add = jnp.where(left, 0.0, m)
            t_h, t_l = split(trans)
            lhs = lanes_of(jnp.where(left, t_h.astype(F32), roll_half(t_l.astype(F32))).astype(BF16), t_h)
            s_h, s_l = split(state[g])
            state[g] = nn(lhs, rows_of(s_h, s_h, s_l, zero)) + add
    starts = [None]
    z = jnp.where(left, roll_half(state[0]), 0.0)
    for g in range(1, groups):
        starts.append(z)
        if g < groups - 1:
            z = jnp.where(left, apply_state(state[g], z, left) + roll_half(state[g]), 0.0)
    for g in range(groups):
        stack = g_ref[g]
        wide = lax.broadcasted_iota(jnp.int32, (64 * per, C), 1) < 64
        total = roll_half(stack)
        if g > 0:
            total = total + apply_state(stack, starts[g], wide)
        for step in range(per):
            zc = total[64 * step : 64 * step + 64]
            packed = jnp.where(left[:32], zc[:32], roll_half(zc[32:]))
            zs_ref[g * per + step] = packed.astype(BF16)


def apply_state(stack, z, left):
    t_h, t_l = split(jnp.where(left, stack, 0.0))
    z_h, z_l = split(z)
    zero = jnp.zeros((64, C), BF16)
    lhs = lanes_of(jnp.where(left, t_h.astype(F32), roll_half(t_l.astype(F32))).astype(BF16), t_h)
    return nn(lhs, rows_of(z_h, z_h, z_l, zero))


GF = GROUP = 4


def group_finish(pairs, z_ref, p_ref, o_ref, gain_ref, mix_ref):
    row, col = iotas()
    left = lax.broadcasted_iota(jnp.int32, (32, C), 1) < 64
    mean_w = jnp.where((row < 64) == (col < 64), 1.0 / 64, 0.0).astype(BF16)
    mean_w = rows_of(mean_w, mean_w)
    reads = []
    for pair in pairs:
        za = z_ref[2 * pair].astype(F32)
        zb = z_ref[2 * pair + 1].astype(F32)
        zw = rows_of(
            jnp.where(left, za, 0.0),
            jnp.where(left, roll_half(za), 0.0),
            jnp.where(left, 0.0, roll_half(zb)),
            jnp.where(left, 0.0, zb),
        ).astype(BF16)
        reads.append(o_ref[pair] + nn(p_ref[pair], rows_of(zw, zw)))
    centred = [r - nn(lanes_of(*split(r)), mean_w) for r in reads]
    var = [nn(lanes_of(*split(c * c)), mean_w) for c in centred]
    for pair, c, v in zip(pairs, centred, var):
        at = pl.ds(pl.multiple_of(pair * C, C), C)
        mix_ref[:, at] = (c * lax.rsqrt(v + 1.0) * gain_ref[pl.ds(pair, 1), :]).astype(BF16)


def project(slot, mix_ref, w_ref, done_ref):
    acc = jnp.zeros((C, 2 * C), F32)
    for k in range(8):
        at = pl.ds(256 * k, 256)
        acc = acc + nn(mix_ref[:, at], lanes_of(w_ref[0, slot, at, :], w_ref[1, slot, at, :]))
    done_ref[slot] = acc.astype(BF16)


def remote(src, dst, send, recv, **where):
    return pltpu.make_async_remote_copy(
        src_ref=src, dst_ref=dst, send_sem=send, recv_sem=recv, device_id=where, device_id_type=MESH
    )


def kernel(
    q_in,
    k_in,
    v_in,
    dl_in,
    rl_in,
    du_in,
    ru_in,
    base_in,
    gain_in,
    weight_ref,
    out_ref,
    q_ref,
    k_ref,
    v_ref,
    dl_ref,
    rl_ref,
    du_ref,
    ru_ref,
    base_ref,
    gain_ref,
    done_ref,
    in_sem,
    out_sem,
    sq_ref,
    msg_ref,
    got_ref,
    group_ref,
    zs_ref,
    zgot_ref,
    p_ref,
    o_ref,
    mix_ref,
    wall_ref,
    f_ref,
    g_ref,
    qs_ref,
    w_ref,
    n_ref,
    own_sem,
    msg_send,
    msg_recv,
    z_send,
    z_recv,
    ring_send,
    ring_recv,
    swap_send,
    swap_recv,
    side_send,
    side_recv,
):
    me = lax.axis_index("sp")
    dp = lax.axis_index("dp")
    core = lax.rem(dp, 2)
    chip = lax.div(dp, 2)
    partner = dp + 1 - 2 * core
    up = lax.rem(dp + 2, DPN)
    down = lax.rem(dp + DPN - 2, DPN)

    inputs = [
        pltpu.make_async_copy(src, dst, in_sem.at[n])
        for n, (src, dst) in enumerate(
            (
                (dl_in, dl_ref),
                (rl_in, rl_ref),
                (du_in, du_ref),
                (ru_in, ru_ref),
                (base_in, base_ref),
                (gain_in, gain_ref),
                (k_in, k_ref),
                (q_in, q_ref),
                (v_in, v_ref),
            )
        )
    ]
    barrier = pltpu.get_barrier_semaphore()

    @pl.loop(1, SP)
    def _(j):
        pl.semaphore_signal(
            barrier, inc=1, device_id={"sp": lax.rem(me + j, SP)}, device_id_type=MESH
        )

    for other in (partner, up, down):
        pl.semaphore_signal(barrier, inc=1, device_id={"dp": other}, device_id_type=MESH)
    own = pltpu.make_async_copy(weight_ref, wall_ref.at[core, 0], own_sem)
    own.start()
    for copy in inputs:
        copy.start()
    inputs[0].wait()
    sq_ref[...] = jnp.tanh(dl_ref[...].astype(F32)).astype(BF16)
    with jax.named_scope("entry"):
        own.wait()
        for copy in inputs[1:]:
            copy.wait()
        pl.semaphore_wait(barrier, SP + 2)

    across = lax.rem(me, 4)
    parity = lax.rem(across, 2)

    def rows(slot, start, count):
        return wall_ref.at[core, slot, pl.ds(pl.multiple_of(start, 16), count), :]

    def ring(way, order):
        near = order // 2
        half = order % 2 if way == 0 else 1 - order % 2
        src, dst = ((YN - near) % YN, YN - 1 - near) if way == 0 else (near, near + 1)
        spans = ((WHOLE // 2 * half, WHOLE // 2), (WHOLE + 2 * PART * parity + PART * half, PART))
        return [
            remote(
                rows(src, *spans[kind]),
                rows(dst, *spans[kind]),
                ring_send.at[kind, way, order],
                ring_recv.at[kind, way, order],
                dp=(up, down)[way],
            )
            for kind in range(2)
        ]

    def swap(hop, slot):
        ref = rows(slot, WHOLE + 2 * PART * parity + PART * hop, PART)
        there = me - across + lax.rem(across + 1 + 2 * hop, 4)
        return remote(ref, ref, swap_send.at[hop, slot], swap_recv.at[hop, slot], sp=there)

    def side(slot, to_me=False):
        start, count = ((0, WHOLE) if slot < YN else (WHOLE, 2048 - WHOLE)) if slot in (4, YN) else (0, 2048)
        ref = wall_ref.at[1 - core if to_me else core, slot % YN if slot < YN else 4, pl.ds(start, count), :]
        return remote(ref, ref, side_send.at[slot], side_recv.at[slot], dp=partner)

    def ring_step(s):
        with jax.named_scope("ring" + str(s)):
            for way in range(2):
                for copy in ring(way, s):
                    copy.wait_recv()
                if s < 5:
                    for copy in ring(way, s + 2):
                        copy.start()

    def share(*slots):
        for slot in slots:
            for hop in range(2):
                swap(hop, slot).start()

    def complete(*slots):
        with jax.named_scope("complete"):
            for slot in slots:
                for hop in range(2):
                    swap(hop, slot).wait_recv()
                side(YN if slot == 4 else slot).start()

    for way in range(2):
        for order in range(2):
            for copy in ring(way, order):
                copy.start()
    side(0).start()

    def send_message(head):
        return remote(
            msg_ref.at[head], got_ref.at[me], msg_send.at[head], msg_recv.at[me], sp=head
        )

    def send_pair(pair):
        for i in range(2):
            head = 2 * pair + i

            @pl.when(head != me)
            def _():
                send_message(head).start()

    first_pair = lax.div(me, 2)
    hold = (f_ref, g_ref, qs_ref, w_ref, n_ref)
    refs = (q_ref, k_ref, v_ref, sq_ref, rl_ref, du_ref, ru_ref, base_ref)

    def pairs_of(i):
        return [lax.rem(first_pair + o, PAIRS) for o in (8 - 2 * i, 9 + 2 * i, 7 - 2 * i, 10 + 2 * i)]

    def send_group(i):
        for pair in pairs_of(i):
            send_pair(pair)

    @pl.loop(0, PAIRS // GROUP)
    def _(i):
        @pl.when(i > 0)
        def _():
            send_group(i - 1)

        @pl.when(i == 2)
        def _():
            ring_step(0)

        @pl.when(i == 3)
        def _():
            ring_step(1)
            share(7, 1)

        with jax.named_scope('group'):
            group_states(pairs_of(i), refs, msg_ref, hold)

    got_ref[me] = msg_ref[me]
    send_group(PAIRS // GROUP - 1)
    ring_step(2)

    def reads(i):
        with jax.named_scope("reads"):
            group_reads([GROUP * i + j for j in range(GROUP)], hold, p_ref, o_ref)

    reads(0)
    reads(1)
    ring_step(3)
    share(6, 2)

    with jax.named_scope('msgwait'):
     @pl.loop(1, SP)
     def _(j):
        other = lax.rem(me + j, SP)
        remote(
            msg_ref.at[me], got_ref.at[other], msg_send.at[other], msg_recv.at[other], sp=other
        ).wait_recv()

    with jax.named_scope('scan'):
        compose_chunks(lax.rem(me, 2) == 1, got_ref, zs_ref, group_ref)

    def send_state(chunk):
        return remote(
            zs_ref.at[chunk], zgot_ref.at[me], z_send.at[chunk], z_recv.at[me], sp=chunk
        )

    zgot_ref[me] = zs_ref[me]

    send_state(lax.rem(me + 16, SP)).start()

    @pl.loop(1, 16)
    def _(j):
        send_state(lax.rem(me + 16 + j, SP)).start()
        send_state(lax.rem(me + 16 - j, SP)).start()

    ring_step(4)
    complete(7, 1)
    reads(2)
    reads(3)

    ring_step(5)
    share(5, 3)

    def wait_state(head):
        @pl.when(head != me)
        def _():
            remote(
                zs_ref.at[me], zgot_ref.at[head], z_send.at[head], z_recv.at[head], sp=head
            ).wait_recv()

    def finish(i):
        with jax.named_scope("zwait"):
            for pair in pairs_of(i):
                wait_state(2 * pair)
                wait_state(2 * pair + 1)
        with jax.named_scope("finish"):
            group_finish(pairs_of(i), zgot_ref, p_ref, o_ref, gain_ref, mix_ref)

    pl.loop(0, 1)(finish)
    complete(6, 2)
    pl.loop(1, 2)(finish)
    ring_step(6)
    share(4)
    side(4).start()
    pl.loop(2, PAIRS // GROUP)(finish)
    complete(5, 3)

    def put_out(slot):
        at = pl.ds(pl.multiple_of(lax.rem(chip + slot, YN) * 256, 256), 256)
        return pltpu.make_async_copy(done_ref.at[slot], out_ref.at[:, at], out_sem.at[slot])

    def project_slots(*slots):
        for slot in slots:
            side(slot, True).wait_recv()
            if slot == 4:
                side(YN, True).wait_recv()
        with jax.named_scope("project"):
            for slot in slots:
                project(slot, mix_ref, wall_ref, done_ref)
                put_out(slot).start()

    project_slots(0, 7, 1)
    complete(4)
    project_slots(6, 2, 5, 3)
    project_slots(4)
    with jax.named_scope("outwait"):
        for slot in range(YN):
            put_out(slot).wait()

    with jax.named_scope("tail"):
        @pl.loop(1, SP)
        def _(j):
            other = lax.rem(me + j, SP)
            send_message(other).wait_send()
            send_state(other).wait_send()

    with jax.named_scope("sent"):
        for way in range(2):
            for order in range(7):
                for copy in ring(way, order):
                    copy.wait_send()
        for slot in range(1, YN):
            for hop in range(2):
                swap(hop, slot).wait_send()
        for slot in range(YN + 1):
            side(slot).wait_send()


def per_device(query, key, value, decay_low, rate_low, decay_up, rate_up, base, gain, weight):
    dma = pltpu.SemaphoreType.DMA
    out = pl.pallas_call(
        kernel,
        out_shape=jax.ShapeDtypeStruct((C, 2048), BF16),
        in_specs=[pl.BlockSpec(memory_space=pl.ANY)] * 10,
        out_specs=pl.BlockSpec(memory_space=pl.ANY),
        scratch_shapes=[
            pltpu.VMEM((C, 2048), BF16),
            pltpu.VMEM((C, 2048), BF16),
            pltpu.VMEM((C, 2048), BF16),
            pltpu.VMEM((C, C), BF16),
            pltpu.VMEM((C, C), BF16),
            pltpu.VMEM((C, 2048), BF16),
            pltpu.VMEM((C, 2048), BF16),
            pltpu.VMEM((PAIRS, C), F32),
            pltpu.VMEM((PAIRS, C), F32),
            pltpu.VMEM((YN, C, 2 * C), BF16),
            dma((9,)),
            dma((YN,)),
            pltpu.VMEM((C, C), BF16),
            pltpu.VMEM((SP, MSG, C), BF16),
            pltpu.VMEM((SP, MSG, C), BF16),
            pltpu.VMEM((4, 512, C), F32),
            pltpu.VMEM((SP, 32, C), BF16),
            pltpu.VMEM((SP, 32, C), BF16),
            pltpu.VMEM((PAIRS, C, 2 * C), BF16),
            pltpu.VMEM((PAIRS, C, C), F32),
            pltpu.VMEM((C, 2048), BF16),
            pltpu.VMEM((2, YN, 2048, C), BF16),
            pltpu.VMEM((PAIRS, C, 2 * C), BF16),
            pltpu.VMEM((PAIRS, 2 * C, 2 * C), BF16),
            pltpu.VMEM((PAIRS, C, C), F32),
            pltpu.VMEM((SP, 2 * C, C), BF16),
            pltpu.VMEM((SP, C, C), BF16),
            dma,
            dma((SP,)),
            dma((SP,)),
            dma((SP,)),
            dma((SP,)),
            dma((2, 2, 7)),
            dma((2, 2, 7)),
            dma((2, YN)),
            dma((2, YN)),
            dma((YN + 1,)),
            dma((YN + 1,)),
        ],
        compiler_params=pltpu.CompilerParams(
            collective_id=0, has_side_effects=True, vmem_limit_bytes=60 * 2**20
        ),
        name="mixer",
    )(
        query[0],
        key[0],
        value[0],
        decay_low[0],
        rate_low[0],
        decay_up,
        rate_up,
        base.reshape(PAIRS, C),
        gain.reshape(PAIRS, C),
        weight,
    )
    return out[None]


def solution(mesh):
    placed = (P("dp", "sp", None),) * 5 + (P(),) * 4 + (P(None, "dp"),)
    return jax.shard_map(
        per_device, mesh=mesh, in_specs=placed, out_specs=P("dp", "sp", None), check_vma=False
    )
```
